32 devices in a mesh: tp: 16 (over z, y, x), dp: 2 (over core).
Axes of the slice: x: 2, y: 2, z: 4, core: 2. Of those that a mesh axis runs over, the one named last changes fastest.
Arguments:
- tokens: bfloat16 [256, 4096], P(None, 'dp'), may hold values from -20 to 20
- norm_gain: float32 [2, 4096], P(None, 'dp'), may hold values from 0.1 to 1.9
- receptance: bfloat16 [2, 4096, 1024], P(None, 'dp', 'tp'), may hold values from -0.09375 to 0.09375
- key_proj: bfloat16 [2, 4096, 1024], P(None, 'dp', 'tp'), may hold values from -0.09375 to 0.09375
- value_proj: bfloat16 [2, 4096, 1024], P(None, 'dp', 'tp'), may hold values from -0.09375 to 0.09375
- decay_proj: bfloat16 [2, 4096, 1024], P(None, 'dp', 'tp'), may hold values from -0.09375 to 0.09375
- rate_proj: bfloat16 [2, 4096, 1024], P(None, 'dp', 'tp'), may hold values from -0.09375 to 0.09375
- gate_proj: bfloat16 [2, 4096, 1024], P(None, 'dp', 'tp'), may hold values from -0.09375 to 0.09375
- decay_base: float32 [2, 1024], P(None, 'tp'), may hold values from -6 to 1
- group_gain: float32 [2, 1024], P(None, 'tp'), may hold values from 0.1 to 1.9
- output_proj: bfloat16 [2, 1024, 4096], P(None, 'tp', 'dp'), may hold values from -0.1875 to 0.1875
- state: float32 [2, 256, 16, 4096], P(None, 'dp', 'tp'), may hold values from -3 to 3
Outputs:
- next_tokens: bfloat16 [256, 4096], P(None, 'dp')
- new_state: float32 [2, 256, 16, 4096], P(None, 'dp', 'tp')
The draws below stay inside these ranges and needn't reach their ends.
All inputs are finite; a program needn't handle non-finite values.
Results may differ from the reference program's by a relative error of at most 0.0066.
Values may be sent and summed in bfloat16 or wider, within the bound.
A program may use at most 64 MiB of HBM per device.

```python
import jax
import jax.numpy as jnp
from jax import lax

D = 4096
HEAD = 64
HEADS = 16
D_ATT = 1024
LAYERS = 2
BATCH = 256


def draw_tokens(key, part):
    base_key, row_key = jax.random.split(key)
    position = jnp.arange(D, dtype=jnp.float32) / D
    feature_scale = 0.4 + 1.6 * position
    row_scale = jnp.exp(jax.random.uniform(row_key, (BATCH, 1), jnp.float32, -0.6, 0.6))
    values = jnp.clip(jax.random.normal(base_key, (BATCH, D), jnp.float32), -5.0, 5.0)
    return (values * feature_scale[None, :] * row_scale).astype(jnp.bfloat16)


def block_levels(stream_key, shape, pieces, low, high):
    def one(axis_at, blocks):
        draws = jax.random.uniform(jax.random.fold_in(jax.random.fold_in(stream_key, 6), axis_at), (blocks,), jnp.float32, low / len(pieces), high / len(pieces))
        return jnp.repeat(jnp.exp(draws), shape[axis_at] // blocks).reshape((-1,) + (1,) * (len(shape) - axis_at - 1))

    level = one(*pieces[0])
    for cut in pieces[1:]:
        level = level * one(*cut)
    return level


def gaussian(stream_key, shape, deviation, limit, cuts=(), held_as=jnp.bfloat16):
    loudness = block_levels(stream_key, shape, cuts, -0.22, 0.18) if cuts else 1.0
    drawn = jax.random.normal(stream_key, shape, jnp.float32) * deviation * loudness
    return jnp.minimum(jnp.maximum(drawn, -limit), limit).astype(held_as)


def setup_inputs(seed: int = 0) -> dict:
    arg_keys = jax.random.split(jax.random.key(seed), 13)
    return {
        "tokens": draw_tokens(jax.random.fold_in(arg_keys[12], 71), 0),
        "norm_gain": jnp.clip(1.0 + 0.18 * jax.random.normal(arg_keys[1], (LAYERS, D), jnp.float32), 0.1, 1.9),
        "receptance": gaussian(arg_keys[2], (LAYERS, D, D_ATT), D ** -0.5, 0.09375, ((1, 2), (2, 16))),
        "key_proj": gaussian(arg_keys[3], (LAYERS, D, D_ATT), D ** -0.5, 0.09375, ((1, 2), (2, 16))),
        "value_proj": gaussian(arg_keys[4], (LAYERS, D, D_ATT), D ** -0.5, 0.09375, ((1, 2), (2, 16))),
        "decay_proj": gaussian(arg_keys[5], (LAYERS, D, D_ATT), D ** -0.5, 0.09375, ((1, 2), (2, 16))),
        "rate_proj": gaussian(arg_keys[6], (LAYERS, D, D_ATT), D ** -0.5, 0.09375, ((1, 2), (2, 16))),
        "gate_proj": gaussian(arg_keys[7], (LAYERS, D, D_ATT), D ** -0.5, 0.09375, ((1, 2), (2, 16))),
        "decay_base": jnp.clip(-6.0 + 7.0 * jax.random.uniform(arg_keys[8], (LAYERS, D_ATT), jnp.float32) ** block_levels(arg_keys[8], (LAYERS, D_ATT), ((1, 16),), -0.2, 0.2), -6.0, 1.0),
        "group_gain": jnp.clip(1.0 + 0.18 * jax.random.normal(arg_keys[9], (LAYERS, D_ATT), jnp.float32), 0.1, 1.9),
        "output_proj": gaussian(arg_keys[10], (LAYERS, D_ATT, D), D_ATT ** -0.5, 0.1875, ((1, 16), (2, 2))),
        "state": gaussian(arg_keys[11], (LAYERS, BATCH, HEADS, HEAD * HEAD), 0.5, 3.0, ((1, 2), (2, 16)), jnp.float32),
    }


norm_floor = 0.1
group_floor = 0.5

def recurrence(state_block, recept_heads, key_heads, value_heads, decay_heads, rate_heads):
    log_rate = -jax.nn.softplus(-decay_heads) - 0.5
    forget = jnp.exp(-jnp.exp(log_rate))
    learn_rate = jax.nn.sigmoid(rate_heads)
    unit_key = key_heads * lax.rsqrt(lax.optimization_barrier(jnp.sum(key_heads * key_heads, axis=-1, keepdims=True)) + 1.0)
    scaled = key_heads * learn_rate
    removed = jnp.einsum('bhvk,bhk->bhv', state_block, -unit_key, precision=lax.Precision.HIGHEST)
    updated = state_block * forget[:, :, None, :] + removed[..., None] * (unit_key * learn_rate)[:, :, None, :] + value_heads[..., None] * scaled[:, :, None, :]
    read_out = jnp.einsum('bhvk,bhk->bhv', updated, recept_heads, precision=lax.Precision.HIGHEST)
    centre = read_out - lax.optimization_barrier(jnp.mean(read_out, axis=-1, keepdims=True))
    normal = centre * lax.rsqrt(lax.optimization_barrier(jnp.mean(centre * centre, axis=-1, keepdims=True)) + group_floor)
    return (updated, normal)

def reference(tokens, norm_gain, receptance, key_proj, value_proj, decay_proj, rate_proj, gate_proj, decay_base, group_gain, output_proj, state):
    current = tokens
    finals = []
    for section_index in range(LAYERS):
        floats = current.astype(jnp.float32)
        squares = lax.optimization_barrier(jnp.sum(floats * floats, axis=1))
        inv_rms = lax.rsqrt(squares / D + norm_floor)
        normed = (floats * norm_gain[section_index]).astype(jnp.bfloat16)

        def by_head(weights):
            term = jnp.dot(normed, weights[section_index], preferred_element_type=jnp.float32)
            rounded = lax.optimization_barrier((inv_rms[:, None] * term).astype(jnp.bfloat16))
            return rounded.astype(jnp.float32).reshape(BATCH, HEADS, HEAD)
        decay_heads = by_head(decay_proj) + decay_base[section_index].reshape(1, HEADS, HEAD)
        updated, normal = recurrence(state[section_index].reshape(BATCH, HEADS, HEAD, HEAD), by_head(receptance), by_head(key_proj), by_head(value_proj), decay_heads, by_head(rate_proj))
        finals.append(updated.reshape(BATCH, HEADS, HEAD * HEAD))
        gate_value = jax.nn.sigmoid(by_head(gate_proj).reshape(BATCH, D_ATT))
        mixed_heads = (normal.reshape(BATCH, D_ATT) * group_gain[section_index] * gate_value).astype(jnp.bfloat16)
        branch = jnp.dot(mixed_heads, output_proj[section_index], preferred_element_type=jnp.float32)
        current = (floats + branch).astype(jnp.bfloat16)
    return (current, jnp.stack(finals))
```

```python
import functools

import jax
import jax.numpy as jnp
from jax import lax
from jax.experimental import pallas as pl
from jax.experimental.pallas import tpu as pltpu
from jax.sharding import PartitionSpec as P

D = 4096
HEAD = 64
LAYERS = 2


norm_floor = 0.1
group_floor = 0.5


def recurrence(state_block, recept_heads, key_heads, value_heads, decay_heads, rate_heads):
    log_rate = -jax.nn.softplus(-decay_heads) - 0.5
    forget = jnp.exp(-jnp.exp(log_rate))
    learn_rate = jax.nn.sigmoid(rate_heads)
    unit_key = key_heads * lax.rsqrt(jnp.sum(key_heads * key_heads, axis=-1, keepdims=True) + 1.0)
    scaled = key_heads * learn_rate
    removed = jnp.einsum("bhvk,bhk->bhv", state_block, -unit_key, precision=lax.Precision.HIGHEST)
    updated = (
        state_block * forget[:, :, None, :]
        + removed[..., None] * (unit_key * learn_rate)[:, :, None, :]
        + value_heads[..., None] * scaled[:, :, None, :]
    )
    read_out = jnp.einsum("bhvk,bhk->bhv", updated, recept_heads, precision=lax.Precision.HIGHEST)
    centre = read_out - jnp.mean(read_out, axis=-1, keepdims=True)
    normal = centre * lax.rsqrt(jnp.mean(centre * centre, axis=-1, keepdims=True) + group_floor)
    return (updated, normal)


def shards(
    tokens,
    norm_gain,
    receptance,
    key_proj,
    value_proj,
    decay_proj,
    rate_proj,
    gate_proj,
    decay_base,
    group_gain,
    output_proj,
    state,
):
    local_rows = state.shape[1]
    first_row = lax.axis_index("dp") * local_rows
    local_heads = state.shape[2]
    current = tokens
    finals = []
    for section_index in range(LAYERS):
        floats = current.astype(jnp.float32)
        squares = jnp.sum(floats * floats, axis=1)
        normed = (floats * norm_gain[section_index]).astype(jnp.bfloat16)
        part_recept = jnp.dot(normed, receptance[section_index], preferred_element_type=jnp.float32)
        part_key = jnp.dot(normed, key_proj[section_index], preferred_element_type=jnp.float32)
        part_value = jnp.dot(normed, value_proj[section_index], preferred_element_type=jnp.float32)
        part_decay = jnp.dot(normed, decay_proj[section_index], preferred_element_type=jnp.float32)
        part_rate = jnp.dot(normed, rate_proj[section_index], preferred_element_type=jnp.float32)
        part_gate = jnp.dot(normed, gate_proj[section_index], preferred_element_type=jnp.float32)
        totals = lax.psum(squares, "dp")
        own_squares = lax.dynamic_slice_in_dim(totals, first_row, local_rows, 0)
        summed = (
            lax.psum_scatter(part_recept, "dp", scatter_dimension=0, tiled=True),
            lax.psum_scatter(part_key, "dp", scatter_dimension=0, tiled=True),
            lax.psum_scatter(part_value, "dp", scatter_dimension=0, tiled=True),
            lax.psum_scatter(part_decay, "dp", scatter_dimension=0, tiled=True),
            lax.psum_scatter(part_rate, "dp", scatter_dimension=0, tiled=True),
            lax.psum_scatter(part_gate, "dp", scatter_dimension=0, tiled=True),
        )
        inv_rms = lax.rsqrt(own_squares / D + norm_floor)

        def by_head(term):
            rounded = lax.optimization_barrier((inv_rms[:, None] * term).astype(jnp.bfloat16))
            return rounded.astype(jnp.float32).reshape(local_rows, local_heads, HEAD)

        decay_heads = by_head(summed[3]) + decay_base[section_index].reshape(1, local_heads, HEAD)
        updated, normal = recurrence(
            state[section_index].reshape(local_rows, local_heads, HEAD, HEAD),
            by_head(summed[0]),
            by_head(summed[1]),
            by_head(summed[2]),
            decay_heads,
            by_head(summed[4]),
        )
        finals.append(updated.reshape(local_rows, local_heads, HEAD * HEAD))
        gate_value = jax.nn.sigmoid(by_head(summed[5]).reshape(local_rows, local_heads * HEAD))
        mixed_heads = (
            normal.reshape(local_rows, local_heads * HEAD) * group_gain[section_index] * gate_value
        ).astype(jnp.bfloat16)
        weights_out = output_proj[section_index]

        def apply_out(piece, begin, weights_out=weights_out):
            return jnp.dot(piece, weights_out, preferred_element_type=jnp.float32)

        partial_out = apply_out(lax.all_gather(mixed_heads, "dp", axis=0, tiled=True), jnp.int32(0))
        total = lax.psum(partial_out, "tp")
        current = (floats + total).astype(jnp.bfloat16)
    return (current, jnp.stack(finals))


MESH = pl.DeviceIdType.MESH
NT = (((1,), (1,)), ((), ()))
PAIR = 2 * HEAD
VMEM_LIMIT = 57 * 1024 * 1024


class Grid:
    def __init__(self, tp):
        self.tp, self.nz, self.per = tp, tp // 4, tp // 2
        self.t, self.d = lax.axis_index("tp"), lax.axis_index("dp")
        self.z = self.t // 4
        x, y = lax.rem(self.t, 2), lax.rem(self.t // 2, 2)
        self.xp, self.yp = self.t + 1 - 2 * x, self.t + 2 - 4 * y
        self.xyp = self.xp + self.yp - self.t
        order = [sorted((k for k in range(self.nz) if k != z), key=lambda k: abs(k - z)) for z in range(self.nz)]
        self.line = []
        for k in range(self.nz - 1):
            level = order[0][k]
            for z in range(1, self.nz):
                level = jnp.where(self.z == z, order[z][k], level)
            self.line.append(level * 4 + lax.rem(self.t, 4))

    def over(self, base, chip):
        return base // 4 * 4 + lax.rem(chip, 4)

    def lots(self):
        return [self.t] + self.line


class Sender:
    def __init__(self, sems):
        self.sems, self.ops = sems, []

    def put(self, src, dst, recv, t, d, when=None):
        op = pltpu.make_async_remote_copy(
            src_ref=src, dst_ref=dst, send_sem=self.sems.at[len(self.ops)], recv_sem=recv,
            device_id={"tp": t, "dp": d}, device_id_type=MESH,
        )
        self.ops.append((op, when))
        if when is None:
            op.start()
        else:
            pl.when(when)(op.start)

    def drain(self):
        for op, when in self.ops:
            if when is None:
                op.wait_send()
            else:
                pl.when(when)(op.wait_send)
        self.ops = []


def landed(ref, recv, grid):
    pltpu.make_async_remote_copy(
        src_ref=ref, dst_ref=ref, send_sem=recv, recv_sem=recv,
        device_id={"tp": grid.xp, "dp": grid.d}, device_id_type=MESH,
    ).wait_recv()


def gather_heads(grid, buf, out, recv, beside):
    def put(block, chip):
        out.put(buf.at[block], buf.at[block], recv.at[block], chip, grid.d)

    for chip in grid.line[::-1] + [grid.xyp, grid.xp, grid.yp]:
        put(grid.t, chip)
    beside()
    for block in grid.line:
        landed(buf.at[block], recv.at[block], grid)
        for chip in (grid.xyp, grid.xp, grid.yp):
            put(block, chip)
    for lot in grid.lots():
        for chip in (grid.xp, grid.yp, grid.xyp):
            block = grid.over(lot, chip)
            landed(buf.at[block], recv.at[block], grid)


def gather_tiles(grid, buf, out, recv, use):
    def put(block, half, chip):
        out.put(buf.at[block, half], buf.at[block, half], recv.at[block, half], chip, grid.d)

    def got(block, half):
        landed(buf.at[block, half], recv.at[block, half], grid)

    def plane(block):
        put(block, 0, grid.xp)
        put(block, 1, grid.yp)
        put(block, 1, grid.xp)
        put(block, 0, grid.yp)

    def relay(lot):
        across, along = grid.over(lot, grid.xp), grid.over(lot, grid.yp)
        got(across, 0)
        put(across, 0, grid.yp)
        got(along, 1)
        put(along, 1, grid.xp)

    for half in range(2):
        for chip in grid.line:
            put(grid.t, half, chip)
    plane(grid.t)
    last = grid.t
    for block in grid.line:
        got(block, 0)
        got(block, 1)
        plane(block)
        relay(last)
        last = block
    relay(last)
    for lot in grid.lots():
        across, along, corner = grid.over(lot, grid.xp), grid.over(lot, grid.yp), grid.over(lot, grid.xyp)
        got(across, 1)
        got(along, 0)
        got(corner, 0)
        got(corner, 1)
        for block in (lot, across, along, corner):
            use(block)


def spread_result(grid, tile, final, out, recv):
    rows, lane = tile.shape[1], tile.shape[2]
    d, per, half_z = grid.d, grid.per, grid.nz // 2
    home = grid.t // per

    def place(block, r, half):
        at = pl.multiple_of((lax.rem(block, per) * 2 + half) * lane, lane)
        return final.at[pl.ds(pl.multiple_of(r * rows, rows), rows), pl.ds(at, lane)]

    def sem(block, r, half):
        return recv.at[lax.rem(block, per), r, half]

    def own(half, chip, when=None):
        out.put(tile.at[half], place(grid.t, d, half), sem(grid.t, d, half), chip, home, when)

    def put(block, r, half, chip, when=None):
        out.put(place(block, r, half), place(block, r, half), sem(block, r, half), chip, d, when)

    def got(block, r, half, when=None):
        def wait():
            landed(place(block, r, half), sem(block, r, half), grid)

        if when is None:
            wait()
        else:
            pl.when(when)(wait)

    away = home != d
    for half in range(2):
        for chip in grid.line:
            own(half, chip)
    own(0, grid.xp)
    own(1, grid.yp)
    own(1, grid.xp)
    own(0, grid.yp)
    for half in range(2):
        own(half, grid.t, away)

        @pl.when(home == d)
        def _(half=half):
            place(grid.t, d, half)[...] = tile[half]

    low = d * half_z
    lots = []
    for k in range(half_z):
        inside = low + lax.rem(grid.z - low + half_z + k, half_z)
        level = jnp.where(grid.z < low, low + k, jnp.where(grid.z >= low + half_z, low + half_z - 1 - k, inside))
        lots.append((level * 4 + lax.rem(grid.t, 4), level != grid.z))

    def relay(lot):
        across, along = grid.over(lot, grid.xp), grid.over(lot, grid.yp)
        for r in range(2):
            got(across, r, 0)
            put(across, r, 0, grid.yp)
            got(along, r, 1)
            put(along, r, 1, grid.xp)

    for lot, far in lots:
        for r in range(2):
            for half in range(2):
                got(lot, r, half, far)
            put(lot, r, 0, grid.xp, far)
            put(lot, r, 1, grid.yp, far)
            put(lot, r, 1, grid.xp, far)
            put(lot, r, 0, grid.yp, far)
        relay(lot)
    for lot, far in lots:
        across, along, corner = grid.over(lot, grid.xp), grid.over(lot, grid.yp), grid.over(lot, grid.xyp)
        for r in range(2):
            for half in range(2):
                got(lot, r, half, jnp.logical_and(jnp.logical_not(far), r != d))
            got(across, r, 1)
            got(along, r, 0)
            got(corner, r, 0)
            got(corner, r, 1)


def iota(shape, axis):
    return lax.broadcasted_iota(jnp.int32, shape, axis)


def update_state(proj, base, ggain, layer, old, new, terms, reads, seqs):
    mine = proj.shape[0]
    lines = old.shape[1] // mine

    def piece(i):
        return proj[:, i * HEAD : (i + 1) * HEAD].astype(jnp.float32)

    recept, key, value, decay, rate = [piece(i) for i in range(5)]
    scale = lax.rsqrt(jnp.sum(key * key, axis=-1, keepdims=True) + 1.0)
    forget = jnp.exp(-jnp.exp(-jax.nn.softplus(-(decay + base[layer : layer + 1, :])) - 0.5))
    learned = key * jax.nn.sigmoid(rate)
    for i, term in enumerate((key * (-scale * scale), forget, learned, recept, value)):
        terms[i] = jnp.concatenate([term, term], axis=-1)

    lane, col = iota((PAIR, PAIR), 0), iota((PAIR, PAIR), 1)
    same = (lane // HEAD == col // HEAD).astype(jnp.bfloat16)
    odd = ((lane < HEAD) & (lane % 2 == col // HEAD)).astype(jnp.bfloat16)
    turn = (lane // HEAD == col % 2).astype(jnp.bfloat16)
    both = jnp.concatenate([same, odd], axis=0)
    mask = (iota((lines, PAIR), 1) % HEAD) // 2 == iota((lines, PAIR), 0)

    def step(i, carry):
        begin = pl.multiple_of(i * seqs, seqs)
        first = pl.multiple_of(i * seqs * lines, seqs * lines)

        def spread(k):
            return jnp.broadcast_to(terms[k, pl.ds(begin, seqs), :][:, None, :], (seqs, lines, PAIR))

        state = old[layer, pl.ds(first, seqs * lines), :].reshape(seqs, lines, PAIR)
        product = (state * spread(0)).astype(jnp.bfloat16).reshape(seqs * lines, PAIR)
        chosen = jnp.where(mask[None], spread(4), 0.0).astype(jnp.bfloat16).reshape(seqs * lines, PAIR)
        rank = jnp.dot(jnp.concatenate([product, chosen], axis=1), both, preferred_element_type=jnp.float32)
        updated = state * spread(1) + rank.reshape(seqs, lines, PAIR) * spread(2)
        new[layer, pl.ds(first, seqs * lines), :] = updated.reshape(seqs * lines, PAIR)
        weighed = (updated * spread(3)).astype(jnp.bfloat16).reshape(seqs * lines, PAIR)
        read = jnp.dot(weighed, turn, preferred_element_type=jnp.float32).reshape(seqs, lines, PAIR)
        reads[pl.ds(begin, seqs), :] = jnp.sum(jnp.where(mask[None], read, 0.0), axis=1)
        return carry

    lax.fori_loop(0, mine // seqs, step, 0)
    read = reads[:, :HEAD]
    centre = read - jnp.mean(read, axis=-1, keepdims=True)
    normal = centre * lax.rsqrt(jnp.mean(centre * centre, axis=-1, keepdims=True) + group_floor)
    return (normal * ggain[layer : layer + 1, :] * jax.nn.sigmoid(piece(5))).astype(jnp.bfloat16)


def whole_kernel(
    tp, tok, gain, wr, wk, wv, wd, wa, wg, wo, base_in, ggain_in, state, final, new,
    tokv, w0, w1, gains, part, inbox, acc, near, outw, we, mg, xg, tile, old, terms, reads, proj, base, ggain,
    load, pair_send, pair_recv, a2a_send, a2a_recv, on_send, on_recv, m_send, m_recv, x_send, x_recv, f_send, f_recv,
):
    grid = Grid(tp)
    t, d, per = grid.t, grid.d, grid.per
    rows, feats = tok.shape
    mine = rows // 2
    cols = near.shape[1]
    width = 6 * HEAD
    weights = (wr, wk, wv, wd, wa, wg)
    here, there = pl.multiple_of(d * mine, mine), pl.multiple_of((1 - d) * mine, mine)

    def copy(src, dst, number):
        return pltpu.make_async_copy(src, dst, load.at[number])

    get_there = copy(tok.at[pl.ds(there, mine)], tokv.at[pl.ds(there, mine)], 0)
    get_here = copy(tok.at[pl.ds(here, mine)], tokv.at[pl.ds(here, mine)], 1)
    get_gain = copy(gain, gains.at[d], 2)
    get_base, get_ggain = copy(base_in, base, 3), copy(ggain_in, ggain, 4)
    get_w0 = [copy(w.at[0], w0.at[pl.ds(i * HEAD, HEAD)], 5 + i) for i, w in enumerate(weights)]
    get_w1 = [copy(w.at[1], w1.at[d, pl.ds(i * HEAD, HEAD)], 11 + i) for i, w in enumerate(weights)]
    get_state = [copy(state.at[k], old.at[k], 17 + k) for k in range(LAYERS)]
    for op in [get_there, get_gain] + get_w0 + [get_here, get_base, get_ggain]:
        op.start()

    barrier = pltpu.get_barrier_semaphore()
    for k in range(1, tp):
        for core in range(2):
            pl.semaphore_signal(barrier, inc=1, device_id={"tp": lax.rem(t + k, tp), "dp": core}, device_id_type=MESH)
    pl.semaphore_signal(barrier, inc=1, device_id={"tp": t, "dp": 1 - d}, device_id_type=MESH)
    for op in [get_state[0]] + get_w1 + [get_state[1]]:
        op.start()

    def project(begin):
        floats = tokv[pl.ds(begin, mine), :].astype(jnp.float32)
        part[pl.ds(begin, mine), width:] = jnp.broadcast_to(jnp.sum(floats * floats, axis=1, keepdims=True), (mine, PAIR))
        normed = (floats * gains[d, 0:1, :]).astype(jnp.bfloat16)
        part[pl.ds(begin, mine), 0:width] = lax.dot_general(normed, w0[...], NT, preferred_element_type=jnp.float32)

    for op in [get_there, get_gain] + get_w0:
        op.wait()
    project(there)
    pl.semaphore_wait(barrier, 2 * tp - 1)

    pair = Sender(pair_send)
    pair.put(part.at[pl.ds(there, mine)], inbox, pair_recv.at[0], t, 1 - d)
    slot = lax.rem(t, per)
    slot_cols = pl.ds(pl.multiple_of(slot * cols, cols), cols)
    pair.put(tokv.at[pl.ds(there, mine), slot_cols], near, pair_recv.at[1], t, 1 - d)
    pair.put(gains.at[d], gains.at[d], pair_recv.at[2], t, 1 - d)

    a2a = [Sender(a2a_send.at[k]) for k in range(LAYERS)]
    home = t // per == d

    def spread_weights(layer):
        for c in range(per):
            block = wo.at[layer, :, pl.ds(c * cols, cols)]
            target = d * per + c
            a2a[layer].put(block, outw.at[layer, t], a2a_recv.at[layer, t], target, d, when=target != t)

            @pl.when(target == t)
            def _(block=block):
                pltpu.make_async_copy(block, outw.at[layer, t], a2a_recv.at[layer, t]).start()

    spread_weights(0)
    for i, w in enumerate(weights):
        block = w1.at[d, pl.ds(i * HEAD, HEAD)]
        pair.put(w.at[1], block, pair_recv.at[3 + i], t, 1 - d)
    spread_weights(1)

    get_here.wait()
    project(here)
    get_base.wait()
    get_ggain.wait()
    landed(inbox, pair_recv.at[0], grid)
    total = part[pl.ds(here, mine), :] + inbox[...]
    inv = lax.rsqrt(total[:, width : width + 1] / (feats * 2) + norm_floor)
    proj[...] = (inv * total[:, :width]).astype(jnp.bfloat16)

    landed(near, pair_recv.at[1], grid)
    own = tokv[pl.ds(here, mine), slot_cols].astype(jnp.float32)
    ours = home.astype(jnp.float32)
    current = own * ours + near[...].astype(jnp.float32) * (1.0 - ours)

    forwards = [Sender(on_send.at[k]) for k in range(LAYERS)]

    def forward_weights(layer):
        for k in range(tp):
            source = lax.rem(t + k, tp)
            block, arrived, onward = outw.at[layer, source], a2a_recv.at[layer, source], on_recv.at[layer, source]
            if k == 0:
                @pl.when(home)
                def _(block=block, arrived=arrived):
                    pltpu.make_async_copy(block, block, arrived).wait()
            else:
                @pl.when(home)
                def _(block=block, arrived=arrived):
                    landed(block, arrived, grid)
            forwards[layer].put(block, block, onward, t, 1 - d, when=home)
        for k in range(tp):
            @pl.when(jnp.logical_not(home))
            def _(k=k):
                landed(outw.at[layer, k], on_recv.at[layer, k], grid)

    def project_out(layer, mixed, current):
        half = mine // 2
        mg[layer, t] = jnp.concatenate([mixed[0:half, :], mixed[half:mine, :]], axis=1)
        heads = Sender(m_send.at[layer])

        def beside():
            forward_weights(layer)
            zero = jnp.zeros((HEAD, cols), we.dtype)
            for k in range(tp):
                block = outw[layer, k]
                top, bottom = pl.ds(k * PAIR, HEAD), pl.ds(k * PAIR + HEAD, HEAD)
                we[top, 0:cols] = block
                we[top, cols : 2 * cols] = zero
                we[bottom, 0:cols] = zero
                we[bottom, cols : 2 * cols] = block

        gather_heads(grid, mg.at[layer], heads, m_recv.at[layer], beside)
        packed = jnp.concatenate([mg[layer, j] for j in range(tp)], axis=1)
        out = jnp.dot(packed, we[...], preferred_element_type=jnp.float32)
        out = jnp.concatenate([out[:, :cols], out[:, cols:]], axis=0)
        heads.drain()
        return (current + out).astype(jnp.bfloat16)

    seqs = min(mine, 16)
    get_state[0].wait()
    mixed = update_state(proj, base, ggain, 0, old, new, terms, reads, seqs)
    stream = project_out(0, mixed, current)

    lane = cols // 2
    for k in range(2):
        xg[t, k] = stream[:, k * lane : (k + 1) * lane]
    for op in get_w1:
        op.wait()
    for i in range(6):
        landed(w1.at[1 - d, pl.ds(i * HEAD, HEAD)], pair_recv.at[3 + i], grid)
    landed(gains.at[1 - d], pair_recv.at[2], grid)
    acc[...] = jnp.zeros(acc.shape, jnp.float32)

    def use(block):
        half, at = block // per, pl.multiple_of(lax.rem(block, per) * cols, cols)
        floats = jnp.concatenate([xg[block, k] for k in range(2)], axis=1).astype(jnp.float32)
        normed = (floats * gains[half, 1:2, pl.ds(at, cols)]).astype(jnp.bfloat16)
        weight = w1[half, :, pl.ds(at, cols)]
        acc[:, 0:width] += lax.dot_general(normed, weight, NT, preferred_element_type=jnp.float32)
        squares = floats * floats
        for k in range(cols // PAIR):
            acc[:, width:] += squares[:, k * PAIR : (k + 1) * PAIR]

    tiles = Sender(x_send)
    gather_tiles(grid, xg, tiles, x_recv, use)
    inv = lax.rsqrt(jnp.sum(acc[:, width:], axis=1, keepdims=True) / (feats * 2) + norm_floor)
    proj[...] = (inv * acc[:, 0:width]).astype(jnp.bfloat16)

    get_state[1].wait()
    mixed = update_state(proj, base, ggain, 1, old, new, terms, reads, seqs)
    stream = project_out(1, mixed, stream.astype(jnp.float32))
    for k in range(2):
        tile[k] = stream[:, k * lane : (k + 1) * lane]
    finish = Sender(f_send)
    spread_result(grid, tile, final, finish, f_recv)

    for sender in [pair, tiles, finish] + a2a + forwards:
        sender.drain()


def store_kernel(final, new, final_out, new_out, sems):
    ops = [pltpu.make_async_copy(new, new_out, sems.at[0]), pltpu.make_async_copy(final, final_out, sems.at[1])]
    for op in ops:
        op.start()
    for op in ops:
        op.wait()


def fast(tp, tokens, norm_gain, projections, decay_base, group_gain, output_proj, state):
    rows, feats = tokens.shape
    mine, per = rows // 2, tp // 2
    cols = feats // per
    width = 6 * HEAD
    lines = HEAD * HEAD // PAIR
    bf, f32 = jnp.bfloat16, jnp.float32
    shape, vmem, dma = jax.ShapeDtypeStruct, pltpu.VMEM, pltpu.SemaphoreType.DMA
    inside, anywhere = pl.BlockSpec(memory_space=pltpu.VMEM), pl.BlockSpec(memory_space=pl.ANY)
    turned = [jnp.swapaxes(w, 1, 2) for w in projections]
    flat = state.reshape(LAYERS, mine * lines, PAIR)
    outs = (shape((rows, feats), bf), shape(flat.shape, f32))
    final, new = pl.pallas_call(
        functools.partial(whole_kernel, tp),
        out_shape=(vmem((rows, feats), bf), vmem(flat.shape, f32)),
        in_specs=[pl.BlockSpec(memory_space=pltpu.HBM)] * 12,
        out_specs=(inside, inside),
        scratch_shapes=[
            vmem((rows, feats), bf), vmem((width, feats), bf), vmem((2, width, feats), bf), vmem((2, LAYERS, feats), f32),
            vmem((rows, width + PAIR), f32), vmem((mine, width + PAIR), f32), vmem((mine, width + PAIR), f32),
            vmem((mine, cols), bf),
            vmem((LAYERS, tp, HEAD, cols), bf), vmem((tp * PAIR, 2 * cols), bf), vmem((LAYERS, tp, mine // 2, PAIR), bf),
            vmem((tp, 2, mine, cols // 2), bf), vmem((2, mine, cols // 2), bf), vmem(flat.shape, f32),
            vmem((5, mine, PAIR), f32), vmem((mine, PAIR), f32), vmem((mine, width), bf),
            vmem((LAYERS, HEAD), f32), vmem((LAYERS, HEAD), f32),
            dma((19,)), dma((9,)), dma((9,)), dma((LAYERS, per)), dma((LAYERS, tp)), dma((LAYERS, tp)), dma((LAYERS, tp)),
            dma((LAYERS, 4 * tp)), dma((LAYERS, tp)), dma((8 * tp,)), dma((tp, 2)), dma((8 * tp,)), dma((per, 2, 2)),
        ],
        compiler_params=pltpu.CompilerParams(collective_id=0, has_side_effects=True, vmem_limit_bytes=VMEM_LIMIT),
        name="whole",
    )(tokens, norm_gain, *turned, output_proj, decay_base, group_gain, flat)
    final, new = pl.pallas_call(
        store_kernel,
        out_shape=outs,
        in_specs=[inside, inside],
        out_specs=(anywhere, anywhere),
        scratch_shapes=[dma((2,))],
        compiler_params=pltpu.CompilerParams(vmem_limit_bytes=1024 * 1024),
        name="store",
    )(final, new)
    return (final, new.reshape(state.shape))


def step(tp, dp, tokens, norm_gain, *rest):
    projections, (decay_base, group_gain, output_proj, state) = rest[:6], rest[6:]
    rows, feats = tokens.shape
    fits = dp == 2 and tp % 8 == 0 and state.shape[2] == 1 and state.shape[1] % 64 == 0 and (feats * dp // tp) % 256 == 0
    if fits:
        return fast(tp, tokens, norm_gain, projections, decay_base, group_gain, output_proj, state)
    return shards(tokens, norm_gain, *rest)


def solution(mesh):
    return jax.shard_map(
        functools.partial(step, mesh.shape["tp"], mesh.shape["dp"]),
        mesh=mesh,
        in_specs=(
            P(None, "dp"),
            P(None, "dp"),
            P(None, "dp", "tp"),
            P(None, "dp", "tp"),
            P(None, "dp", "tp"),
            P(None, "dp", "tp"),
            P(None, "dp", "tp"),
            P(None, "dp", "tp"),
            P(None, "tp"),
            P(None, "tp"),
            P(None, "tp", "dp"),
            P(None, "dp", "tp", None),
        ),
        out_specs=(P(None, "dp"), P(None, "dp", "tp", None)),
        check_vma=False,
    )
```

```python
import functools

import jax
import jax.numpy as jnp
from jax import lax
from jax.experimental import pallas as pl
from jax.experimental.pallas import tpu as pltpu
from jax.sharding import PartitionSpec as P

D = 4096
HEAD = 64
LAYERS = 2


norm_floor = 0.1
group_floor = 0.5


def recurrence(state_block, recept_heads, key_heads, value_heads, decay_heads, rate_heads):
    log_rate = -jax.nn.softplus(-decay_heads) - 0.5
    forget = jnp.exp(-jnp.exp(log_rate))
    learn_rate = jax.nn.sigmoid(rate_heads)
    unit_key = key_heads * lax.rsqrt(jnp.sum(key_heads * key_heads, axis=-1, keepdims=True) + 1.0)
    scaled = key_heads * learn_rate
    removed = jnp.einsum("bhvk,bhk->bhv", state_block, -unit_key, precision=lax.Precision.HIGHEST)
    updated = (
        state_block * forget[:, :, None, :]
        + removed[..., None] * (unit_key * learn_rate)[:, :, None, :]
        + value_heads[..., None] * scaled[:, :, None, :]
    )
    read_out = jnp.einsum("bhvk,bhk->bhv", updated, recept_heads, precision=lax.Precision.HIGHEST)
    centre = read_out - jnp.mean(read_out, axis=-1, keepdims=True)
    normal = centre * lax.rsqrt(jnp.mean(centre * centre, axis=-1, keepdims=True) + group_floor)
    return (updated, normal)


def shards(
    tokens,
    norm_gain,
    receptance,
    key_proj,
    value_proj,
    decay_proj,
    rate_proj,
    gate_proj,
    decay_base,
    group_gain,
    output_proj,
    state,
):
    local_rows = state.shape[1]
    first_row = lax.axis_index("dp") * local_rows
    local_heads = state.shape[2]
    current = tokens
    finals = []
    for section_index in range(LAYERS):
        floats = current.astype(jnp.float32)
        squares = jnp.sum(floats * floats, axis=1)
        normed = (floats * norm_gain[section_index]).astype(jnp.bfloat16)
        part_recept = jnp.dot(normed, receptance[section_index], preferred_element_type=jnp.float32)
        part_key = jnp.dot(normed, key_proj[section_index], preferred_element_type=jnp.float32)
        part_value = jnp.dot(normed, value_proj[section_index], preferred_element_type=jnp.float32)
        part_decay = jnp.dot(normed, decay_proj[section_index], preferred_element_type=jnp.float32)
        part_rate = jnp.dot(normed, rate_proj[section_index], preferred_element_type=jnp.float32)
        part_gate = jnp.dot(normed, gate_proj[section_index], preferred_element_type=jnp.float32)
        totals = lax.psum(squares, "dp")
        own_squares = lax.dynamic_slice_in_dim(totals, first_row, local_rows, 0)
        summed = (
            lax.psum_scatter(part_recept, "dp", scatter_dimension=0, tiled=True),
            lax.psum_scatter(part_key, "dp", scatter_dimension=0, tiled=True),
            lax.psum_scatter(part_value, "dp", scatter_dimension=0, tiled=True),
            lax.psum_scatter(part_decay, "dp", scatter_dimension=0, tiled=True),
            lax.psum_scatter(part_rate, "dp", scatter_dimension=0, tiled=True),
            lax.psum_scatter(part_gate, "dp", scatter_dimension=0, tiled=True),
        )
        inv_rms = lax.rsqrt(own_squares / D + norm_floor)

        def by_head(term):
            rounded = lax.optimization_barrier((inv_rms[:, None] * term).astype(jnp.bfloat16))
            return rounded.astype(jnp.float32).reshape(local_rows, local_heads, HEAD)

        decay_heads = by_head(summed[3]) + decay_base[section_index].reshape(1, local_heads, HEAD)
        updated, normal = recurrence(
            state[section_index].reshape(local_rows, local_heads, HEAD, HEAD),
            by_head(summed[0]),
            by_head(summed[1]),
            by_head(summed[2]),
            decay_heads,
            by_head(summed[4]),
        )
        finals.append(updated.reshape(local_rows, local_heads, HEAD * HEAD))
        gate_value = jax.nn.sigmoid(by_head(summed[5]).reshape(local_rows, local_heads * HEAD))
        mixed_heads = (
            normal.reshape(local_rows, local_heads * HEAD) * group_gain[section_index] * gate_value
        ).astype(jnp.bfloat16)
        weights_out = output_proj[section_index]

        def apply_out(piece, begin, weights_out=weights_out):
            return jnp.dot(piece, weights_out, preferred_element_type=jnp.float32)

        partial_out = apply_out(lax.all_gather(mixed_heads, "dp", axis=0, tiled=True), jnp.int32(0))
        total = lax.psum(partial_out, "tp")
        current = (floats + total).astype(jnp.bfloat16)
    return (current, jnp.stack(finals))


MESH = pl.DeviceIdType.MESH
NT = (((1,), (1,)), ((), ()))
PAIR = 2 * HEAD
VMEM_LIMIT = 57 * 1024 * 1024


class Grid:
    def __init__(self, tp):
        self.tp, self.nz, self.per = tp, tp // 4, tp // 2
        self.t, self.d = lax.axis_index("tp"), lax.axis_index("dp")
        self.z = self.t // 4
        x, y = lax.rem(self.t, 2), lax.rem(self.t // 2, 2)
        self.xp, self.yp = self.t + 1 - 2 * x, self.t + 2 - 4 * y
        self.xyp = self.xp + self.yp - self.t
        order = [sorted((k for k in range(self.nz) if k != z), key=lambda k: abs(k - z)) for z in range(self.nz)]
        self.line = []
        for k in range(self.nz - 1):
            level = order[0][k]
            for z in range(1, self.nz):
                level = jnp.where(self.z == z, order[z][k], level)
            self.line.append(level * 4 + lax.rem(self.t, 4))

    def over(self, base, chip):
        return base // 4 * 4 + lax.rem(chip, 4)

    def lots(self):
        return [self.t] + self.line


class Sender:
    def __init__(self, sem):
        self.sem = sem

    def put(self, src, dst, recv, t, d, when=None):
        op = pltpu.make_async_remote_copy(
            src_ref=src, dst_ref=dst, send_sem=self.sem, recv_sem=recv,
            device_id={"tp": t, "dp": d}, device_id_type=MESH,
        )
        if when is None:
            op.start()
        else:
            pl.when(when)(op.start)


def whole_of(ref, sem, grid):
    return pltpu.make_async_remote_copy(
        src_ref=ref, dst_ref=ref, send_sem=sem, recv_sem=sem,
        device_id={"tp": grid.xp, "dp": grid.d}, device_id_type=MESH,
    )


def landed(ref, recv, grid, when=None):
    op = whole_of(ref, recv, grid)
    if when is None:
        op.wait_recv()
    else:
        pl.when(when)(op.wait_recv)


def left(ref, send, grid, when=None):
    op = whole_of(ref, send, grid)
    if when is None:
        op.wait_send()
    else:
        pl.when(when)(op.wait_send)


def gather_heads(grid, buf, send, line, plane, beside):
    out = Sender(send)
    for chip in grid.line[::-1]:
        out.put(buf.at[grid.t], buf.at[grid.t], line.at[grid.z], chip, grid.d)
    for chip in (grid.xyp, grid.xp, grid.yp):
        out.put(buf.at[grid.t], buf.at[grid.t], plane, chip, grid.d)
    beside()
    for block in grid.line:
        landed(buf.at[block], line.at[block // 4], grid)
        for chip in (grid.xyp, grid.xp, grid.yp):
            out.put(buf.at[block], buf.at[block], plane, chip, grid.d)
    landed(buf.at[0 : 3 * grid.nz], plane, grid)
    left(buf.at[0 : 4 * grid.nz - 1], send, grid)


def gather_tiles(grid, buf, send, line, relayed, rest, after, use):
    out = Sender(send)

    def put(block, half, recv, chip):
        out.put(buf.at[block, half], buf.at[block, half], recv, chip, grid.d)

    def plane(block):
        level = block // 4
        put(block, 0, relayed.at[level, 0], grid.xp)
        put(block, 1, relayed.at[level, 1], grid.yp)
        put(block, 1, rest.at[level], grid.xp)
        put(block, 0, rest.at[level], grid.yp)

    def relay(lot):
        across, along, level = grid.over(lot, grid.xp), grid.over(lot, grid.yp), lot // 4
        landed(buf.at[across, 0], relayed.at[level, 0], grid)
        put(across, 0, rest.at[level], grid.yp)
        landed(buf.at[along, 1], relayed.at[level, 1], grid)
        put(along, 1, rest.at[level], grid.xp)

    for half in range(2):
        for chip in grid.line:
            put(grid.t, half, line.at[grid.z], chip)
    plane(grid.t)
    last = grid.t
    for block in grid.line:
        landed(buf.at[block], line.at[block // 4], grid)
        plane(block)
        relay(last)
        last = block
    relay(last)
    after()
    for lot in grid.lots():
        landed(buf.at[0:2], rest.at[lot // 4], grid)
        for block in (lot, grid.over(lot, grid.xp), grid.over(lot, grid.yp), grid.over(lot, grid.xyp)):
            use(block)

    def finish():
        left(buf.at[0 : 4 * grid.nz - 1], send, grid)

    return finish


def spread_result(grid, tile, final, send, line, relayed, rest):
    rows, lane = tile.shape[1], tile.shape[2]
    d, per, half_z = grid.d, grid.per, grid.nz // 2
    home = grid.t // per
    out, extra = Sender(send.at[0]), Sender(send.at[1])

    def place(block, r, half):
        at = pl.multiple_of((lax.rem(block, per) * 2 + half) * lane, lane)
        return final.at[pl.ds(pl.multiple_of(r * rows, rows), rows), pl.ds(at, lane)]

    def share(count):
        return final.at[pl.ds(0, count * rows // (2 * per))]

    def deep(block):
        return lax.rem(block // 4, half_z)

    def own(half, recv, chip, when=None):
        (out if when is None else extra).put(tile.at[half], place(grid.t, d, half), recv, chip, home, when)

    away = home != d
    level = deep(grid.t)
    for half in range(2):
        for chip in grid.line:
            own(half, line.at[level, d], chip)
    own(0, relayed.at[level, d, 0], grid.xp)
    own(1, relayed.at[level, d, 1], grid.yp)
    own(1, rest.at[0], grid.xp)
    own(0, rest.at[0], grid.yp)
    for half in range(2):
        own(half, rest.at[1], grid.t, away)

        @pl.when(home == d)
        def _(half=half):
            place(grid.t, d, half)[...] = tile[half]

    low = d * half_z
    lots = []
    for k in range(half_z):
        inside = low + lax.rem(grid.z - low + half_z + k, half_z)
        at = jnp.where(grid.z < low, low + k, jnp.where(grid.z >= low + half_z, low + half_z - 1 - k, inside))
        lots.append((at * 4 + lax.rem(grid.t, 4), at != grid.z))

    def put(block, r, half, recv, chip, far=None):
        (out if far is None else extra).put(place(block, r, half), place(block, r, half), recv, chip, d, far)

    def plane(lot, far):
        level = deep(lot)
        for r in range(2):
            landed(share(2), line.at[level, r], grid, far)
            put(lot, r, 0, relayed.at[level, r, 0], grid.xp, far)
            put(lot, r, 1, relayed.at[level, r, 1], grid.yp, far)
            put(lot, r, 1, rest.at[0], grid.xp, far)
            put(lot, r, 0, rest.at[0], grid.yp, far)

    def relay(lot):
        across, along, level = grid.over(lot, grid.xp), grid.over(lot, grid.yp), deep(lot)
        for r in range(2):
            landed(place(across, r, 0), relayed.at[level, r, 0], grid)
            put(across, r, 0, rest.at[0], grid.yp)
            landed(place(along, r, 1), relayed.at[level, r, 1], grid)
            put(along, r, 1, rest.at[0], grid.xp)

    for lot, far in lots:
        plane(lot, far)
        relay(lot)
    landed(share(8 * half_z), rest.at[0], grid)
    landed(share(2), rest.at[1], grid, home_is(grid))
    left(share(2 * (grid.nz - 1) + 4 + 4 * half_z), send.at[0], grid)
    left(share(2), send.at[1], grid, away)
    for lot, far in lots:
        left(share(8), send.at[1], grid, far)


def home_is(grid):
    return grid.t // grid.per == grid.d


def iota(shape, axis):
    return lax.broadcasted_iota(jnp.int32, shape, axis)


def update_state(proj, base, ggain, layer, old, new, terms, reads, seqs):
    mine = proj.shape[0]
    lines = old.shape[1] // mine

    def piece(i):
        return proj[:, i * HEAD : (i + 1) * HEAD].astype(jnp.float32)

    recept, key, value, decay, rate = [piece(i) for i in range(5)]
    scale = lax.rsqrt(jnp.sum(key * key, axis=-1, keepdims=True) + 1.0)
    forget = jnp.exp(-jnp.exp(-jax.nn.softplus(-(decay + base[layer : layer + 1, :])) - 0.5))
    learned = key * jax.nn.sigmoid(rate)
    for i, term in enumerate((key * (-scale * scale), forget, learned, recept, value)):
        terms[i] = jnp.concatenate([term, term], axis=-1)

    lane, col = iota((PAIR, PAIR), 0), iota((PAIR, PAIR), 1)
    same = (lane // HEAD == col // HEAD).astype(jnp.bfloat16)
    odd = ((lane < HEAD) & (lane % 2 == col // HEAD)).astype(jnp.bfloat16)
    turn = (lane // HEAD == col % 2).astype(jnp.bfloat16)
    both = jnp.concatenate([same, odd], axis=0)
    mask = (iota((lines, PAIR), 1) % HEAD) // 2 == iota((lines, PAIR), 0)

    def step(i, carry):
        begin = pl.multiple_of(i * seqs, seqs)
        first = pl.multiple_of(i * seqs * lines, seqs * lines)

        def spread(k):
            return jnp.broadcast_to(terms[k, pl.ds(begin, seqs), :][:, None, :], (seqs, lines, PAIR))

        state = old[layer, pl.ds(first, seqs * lines), :].reshape(seqs, lines, PAIR)
        product = (state * spread(0)).astype(jnp.bfloat16).reshape(seqs * lines, PAIR)
        chosen = jnp.where(mask[None], spread(4), 0.0).astype(jnp.bfloat16).reshape(seqs * lines, PAIR)
        rank = jnp.dot(jnp.concatenate([product, chosen], axis=1), both, preferred_element_type=jnp.float32)
        updated = state * spread(1) + rank.reshape(seqs, lines, PAIR) * spread(2)
        new[layer, pl.ds(first, seqs * lines), :] = updated.reshape(seqs * lines, PAIR)
        weighed = (updated * spread(3)).astype(jnp.bfloat16).reshape(seqs * lines, PAIR)
        read = jnp.dot(weighed, turn, preferred_element_type=jnp.float32).reshape(seqs, lines, PAIR)
        reads[pl.ds(begin, seqs), :] = jnp.sum(jnp.where(mask[None], read, 0.0), axis=1)
        return carry

    lax.fori_loop(0, mine // seqs, step, 0)
    read = reads[:, :HEAD]
    centre = read - jnp.mean(read, axis=-1, keepdims=True)
    normal = centre * lax.rsqrt(jnp.mean(centre * centre, axis=-1, keepdims=True) + group_floor)
    return (normal * ggain[layer : layer + 1, :] * jax.nn.sigmoid(piece(5))).astype(jnp.bfloat16)


def whole_kernel(
    tp, tok, gain, wr, wk, wv, wd, wa, wg, wo, base_in, ggain_in, state, final, new,
    tokv, w0, w1, gains, part, inbox, acc, near, outw, we, mg, xg, tile, old, terms, reads, proj, base, ggain,
    load, pair_send, pair_recv, a2a_send, a2a_recv, on_send, on_recv, m_send, m_line, m_plane,
    x_send, x_line, x_relayed, x_rest, f_send, f_line, f_relayed, f_rest,
):
    grid = Grid(tp)
    t, d, per = grid.t, grid.d, grid.per
    rows, feats = tok.shape
    mine = rows // 2
    cols = near.shape[1]
    width = 6 * HEAD
    weights = (wr, wk, wv, wd, wa, wg)
    here, there = pl.multiple_of(d * mine, mine), pl.multiple_of((1 - d) * mine, mine)

    def copy(src, dst, number):
        return pltpu.make_async_copy(src, dst, load.at[number])

    get_there = copy(tok.at[pl.ds(there, mine)], tokv.at[pl.ds(there, mine)], 0)
    get_here = copy(tok.at[pl.ds(here, mine)], tokv.at[pl.ds(here, mine)], 1)
    get_gain = copy(gain, gains.at[d], 2)
    get_base, get_ggain = copy(base_in, base, 3), copy(ggain_in, ggain, 4)
    get_w0 = [copy(w.at[0], w0.at[pl.ds(i * HEAD, HEAD)], 5) for i, w in enumerate(weights)]
    get_w1 = [copy(w.at[1], w1.at[d, pl.ds(i * HEAD, HEAD)], 6) for i, w in enumerate(weights)]
    get_state = [copy(state.at[k], old.at[k], 7 + k) for k in range(LAYERS)]
    for op in [get_there, get_gain] + get_w0 + [get_here, get_base, get_ggain]:
        op.start()

    barrier = pltpu.get_barrier_semaphore()
    for k in range(1, tp):
        for core in range(2):
            pl.semaphore_signal(barrier, inc=1, device_id={"tp": lax.rem(t + k, tp), "dp": core}, device_id_type=MESH)
    pl.semaphore_signal(barrier, inc=1, device_id={"tp": t, "dp": 1 - d}, device_id_type=MESH)
    for op in [get_state[0]] + get_w1 + [get_state[1]]:
        op.start()

    def project(begin):
        floats = tokv[pl.ds(begin, mine), :].astype(jnp.float32)
        part[pl.ds(begin, mine), width:] = jnp.broadcast_to(jnp.sum(floats * floats, axis=1, keepdims=True), (mine, PAIR))
        normed = (floats * gains[d, 0:1, :]).astype(jnp.bfloat16)
        part[pl.ds(begin, mine), 0:width] = lax.dot_general(normed, w0[...], NT, preferred_element_type=jnp.float32)

    get_there.wait()
    get_gain.wait()
    copy(w0, w0, 5).wait()
    project(there)
    pl.semaphore_wait(barrier, 2 * tp - 1)

    def to_partner(number, src, dst):
        Sender(pair_send.at[number]).put(src, dst, pair_recv.at[number], t, 1 - d)

    slot = lax.rem(t, per)
    slot_cols = pl.ds(pl.multiple_of(slot * cols, cols), cols)
    to_partner(0, part.at[pl.ds(there, mine)], inbox)
    to_partner(1, tokv.at[pl.ds(there, mine), slot_cols], near)
    to_partner(2, gains.at[d], gains.at[d])

    home = home_is(grid)

    def spread_weights(layer):
        for c in range(per):
            block = wo.at[layer, :, pl.ds(c * cols, cols)]
            target = d * per + c
            Sender(a2a_send.at[layer]).put(block, outw.at[layer, t], a2a_recv.at[layer], target, d, when=target != t)

            @pl.when(target == t)
            def _(block=block):
                pltpu.make_async_copy(block, outw.at[layer, t], a2a_recv.at[layer]).start()

    def weights_left(layer):
        left(outw.at[layer, 0:per], a2a_send.at[layer], grid, jnp.logical_not(home))
        left(outw.at[layer, 0 : per - 1], a2a_send.at[layer], grid, home)
        left(outw.at[layer], on_send.at[layer], grid, home)

    spread_weights(0)
    for i, w in enumerate(weights):
        to_partner(3, w.at[1], w1.at[d, pl.ds(i * HEAD, HEAD)])

    get_here.wait()
    project(here)
    get_base.wait()
    get_ggain.wait()
    landed(inbox, pair_recv.at[0], grid)
    total = part[pl.ds(here, mine), :] + inbox[...]
    inv = lax.rsqrt(total[:, width : width + 1] / (feats * 2) + norm_floor)
    proj[...] = (inv * total[:, :width]).astype(jnp.bfloat16)

    landed(near, pair_recv.at[1], grid)
    own = tokv[pl.ds(here, mine), slot_cols].astype(jnp.float32)
    ours = home.astype(jnp.float32)
    current = own * ours + near[...].astype(jnp.float32) * (1.0 - ours)

    def forward_weights(layer):
        landed(outw.at[layer], a2a_recv.at[layer], grid, home)
        Sender(on_send.at[layer]).put(outw.at[layer], outw.at[layer], on_recv.at[layer], t, 1 - d, when=home)
        landed(outw.at[layer], on_recv.at[layer], grid, jnp.logical_not(home))

    def project_out(layer, mixed, current):
        half = mine // 2
        mg[layer, t] = jnp.concatenate([mixed[0:half, :], mixed[half:mine, :]], axis=1)

        def beside():
            forward_weights(layer)
            zero = jnp.zeros((HEAD, cols), we.dtype)
            for k in range(tp):
                block = outw[layer, k]
                top, bottom = pl.ds(k * PAIR, HEAD), pl.ds(k * PAIR + HEAD, HEAD)
                we[top, 0:cols] = block
                we[top, cols : 2 * cols] = zero
                we[bottom, 0:cols] = zero
                we[bottom, cols : 2 * cols] = block

        gather_heads(grid, mg.at[layer], m_send.at[layer], m_line.at[layer], m_plane.at[layer], beside)
        packed = jnp.concatenate([mg[layer, j] for j in range(tp)], axis=1)
        out = jnp.dot(packed, we[...], preferred_element_type=jnp.float32)
        out = jnp.concatenate([out[:, :cols], out[:, cols:]], axis=0)
        return (current + out).astype(jnp.bfloat16)

    seqs = min(mine, 16)
    get_state[0].wait()
    mixed = update_state(proj, base, ggain, 0, old, new, terms, reads, seqs)
    stream = project_out(0, mixed, current)

    lane = cols // 2
    for k in range(2):
        xg[t, k] = stream[:, k * lane : (k + 1) * lane]
    copy(w1.at[d], w1.at[d], 6).wait()
    landed(w1.at[1 - d], pair_recv.at[3], grid)
    landed(gains.at[1 - d], pair_recv.at[2], grid)
    acc[...] = jnp.zeros(acc.shape, jnp.float32)

    def use(block):
        half, at = block // per, pl.multiple_of(lax.rem(block, per) * cols, cols)
        floats = jnp.concatenate([xg[block, k] for k in range(2)], axis=1).astype(jnp.float32)
        normed = (floats * gains[half, 1:2, pl.ds(at, cols)]).astype(jnp.bfloat16)
        weight = w1[half, :, pl.ds(at, cols)]
        acc[:, 0:width] += lax.dot_general(normed, weight, NT, preferred_element_type=jnp.float32)
        squares = floats * floats
        for k in range(cols // PAIR):
            acc[:, width:] += squares[:, k * PAIR : (k + 1) * PAIR]

    def later():
        spread_weights(1)

    tiles_left = gather_tiles(grid, xg, x_send, x_line, x_relayed, x_rest, later, use)
    inv = lax.rsqrt(jnp.sum(acc[:, width:], axis=1, keepdims=True) / (feats * 2) + norm_floor)
    proj[...] = (inv * acc[:, 0:width]).astype(jnp.bfloat16)

    get_state[1].wait()
    mixed = update_state(proj, base, ggain, 1, old, new, terms, reads, seqs)
    stream = project_out(1, mixed, stream.astype(jnp.float32))
    for k in range(2):
        tile[k] = stream[:, k * lane : (k + 1) * lane]
    spread_result(grid, tile, final, f_send, f_line, f_relayed, f_rest)

    tiles_left()
    left(part.at[pl.ds(there, mine)], pair_send.at[0], grid)
    left(near, pair_send.at[1], grid)
    left(gains.at[d], pair_send.at[2], grid)
    left(w1.at[d], pair_send.at[3], grid)
    for layer in range(LAYERS):
        weights_left(layer)


def store_kernel(final, new, final_out, new_out, sems):
    ops = [pltpu.make_async_copy(new, new_out, sems.at[0]), pltpu.make_async_copy(final, final_out, sems.at[1])]
    for op in ops:
        op.start()
    for op in ops:
        op.wait()


def fast(tp, tokens, norm_gain, projections, decay_base, group_gain, output_proj, state):
    rows, feats = tokens.shape
    mine, per = rows // 2, tp // 2
    cols = feats // per
    width = 6 * HEAD
    lines = HEAD * HEAD // PAIR
    bf, f32 = jnp.bfloat16, jnp.float32
    shape, vmem, dma = jax.ShapeDtypeStruct, pltpu.VMEM, pltpu.SemaphoreType.DMA
    inside, anywhere = pl.BlockSpec(memory_space=pltpu.VMEM), pl.BlockSpec(memory_space=pl.ANY)
    turned = [jnp.swapaxes(w, 1, 2) for w in projections]
    flat = state.reshape(LAYERS, mine * lines, PAIR)
    outs = (shape((rows, feats), bf), shape(flat.shape, f32))
    final, new = pl.pallas_call(
        functools.partial(whole_kernel, tp),
        out_shape=(vmem((rows, feats), bf), vmem(flat.shape, f32)),
        in_specs=[pl.BlockSpec(memory_space=pltpu.HBM)] * 12,
        out_specs=(inside, inside),
        scratch_shapes=[
            vmem((rows, feats), bf), vmem((width, feats), bf), vmem((2, width, feats), bf), vmem((2, LAYERS, feats), f32),
            vmem((rows, width + PAIR), f32), vmem((mine, width + PAIR), f32), vmem((mine, width + PAIR), f32),
            vmem((mine, cols), bf),
            vmem((LAYERS, tp, HEAD, cols), bf), vmem((tp * PAIR, 2 * cols), bf), vmem((LAYERS, tp, mine // 2, PAIR), bf),
            vmem((tp, 2, mine, cols // 2), bf), vmem((2, mine, cols // 2), bf), vmem(flat.shape, f32),
            vmem((5, mine, PAIR), f32), vmem((mine, PAIR), f32), vmem((mine, width), bf),
            vmem((LAYERS, HEAD), f32), vmem((LAYERS, HEAD), f32),
            dma((9,)), dma((4,)), dma((4,)), dma((LAYERS,)), dma((LAYERS,)), dma((LAYERS,)), dma((LAYERS,)),
            dma((LAYERS,)), dma((LAYERS, tp // 4)), dma((LAYERS,)),
            dma, dma((tp // 4,)), dma((tp // 4, 2)), dma((tp // 4,)),
            dma((2,)), dma((tp // 8, 2)), dma((tp // 8, 2, 2)), dma((2,)),
        ],
        compiler_params=pltpu.CompilerParams(collective_id=0, has_side_effects=True, vmem_limit_bytes=VMEM_LIMIT),
        name="whole",
    )(tokens, norm_gain, *turned, output_proj, decay_base, group_gain, flat)
    final, new = pl.pallas_call(
        store_kernel,
        out_shape=outs,
        in_specs=[inside, inside],
        out_specs=(anywhere, anywhere),
        scratch_shapes=[dma((2,))],
        compiler_params=pltpu.CompilerParams(vmem_limit_bytes=1024 * 1024),
        name="store",
    )(final, new)
    return (final, new.reshape(state.shape))


def step(tp, dp, tokens, norm_gain, *rest):
    projections, (decay_base, group_gain, output_proj, state) = rest[:6], rest[6:]
    rows, feats = tokens.shape
    fits = dp == 2 and tp % 8 == 0 and state.shape[2] == 1 and state.shape[1] % 64 == 0 and (feats * dp // tp) % 256 == 0
    if fits:
        return fast(tp, tokens, norm_gain, projections, decay_base, group_gain, output_proj, state)
    return shards(tokens, norm_gain, *rest)


def solution(mesh):
    return jax.shard_map(
        functools.partial(step, mesh.shape["tp"], mesh.shape["dp"]),
        mesh=mesh,
        in_specs=(
            P(None, "dp"),
            P(None, "dp"),
            P(None, "dp", "tp"),
            P(None, "dp", "tp"),
            P(None, "dp", "tp"),
            P(None, "dp", "tp"),
            P(None, "dp", "tp"),
            P(None, "dp", "tp"),
            P(None, "tp"),
            P(None, "tp"),
            P(None, "tp", "dp"),
            P(None, "dp", "tp", None),
        ),
        out_specs=(P(None, "dp"), P(None, "dp", "tp", None)),
        check_vma=False,
    )
```

```python
import functools

import jax
import jax.numpy as jnp
from jax import lax
from jax.experimental import pallas as pl
from jax.experimental.pallas import tpu as pltpu
from jax.sharding import PartitionSpec as P

D = 4096
HEAD = 64
LAYERS = 2


norm_floor = 0.1
group_floor = 0.5


def recurrence(state_block, recept_heads, key_heads, value_heads, decay_heads, rate_heads):
    log_rate = -jax.nn.softplus(-decay_heads) - 0.5
    forget = jnp.exp(-jnp.exp(log_rate))
    learn_rate = jax.nn.sigmoid(rate_heads)
    unit_key = key_heads * lax.rsqrt(jnp.sum(key_heads * key_heads, axis=-1, keepdims=True) + 1.0)
    scaled = key_heads * learn_rate
    removed = jnp.einsum("bhvk,bhk->bhv", state_block, -unit_key, precision=lax.Precision.HIGHEST)
    updated = (
        state_block * forget[:, :, None, :]
        + removed[..., None] * (unit_key * learn_rate)[:, :, None, :]
        + value_heads[..., None] * scaled[:, :, None, :]
    )
    read_out = jnp.einsum("bhvk,bhk->bhv", updated, recept_heads, precision=lax.Precision.HIGHEST)
    centre = read_out - jnp.mean(read_out, axis=-1, keepdims=True)
    normal = centre * lax.rsqrt(jnp.mean(centre * centre, axis=-1, keepdims=True) + group_floor)
    return (updated, normal)


def shards(
    tokens,
    norm_gain,
    receptance,
    key_proj,
    value_proj,
    decay_proj,
    rate_proj,
    gate_proj,
    decay_base,
    group_gain,
    output_proj,
    state,
):
    local_rows = state.shape[1]
    first_row = lax.axis_index("dp") * local_rows
    local_heads = state.shape[2]
    current = tokens
    finals = []
    for section_index in range(LAYERS):
        floats = current.astype(jnp.float32)
        squares = jnp.sum(floats * floats, axis=1)
        normed = (floats * norm_gain[section_index]).astype(jnp.bfloat16)
        part_recept = jnp.dot(normed, receptance[section_index], preferred_element_type=jnp.float32)
        part_key = jnp.dot(normed, key_proj[section_index], preferred_element_type=jnp.float32)
        part_value = jnp.dot(normed, value_proj[section_index], preferred_element_type=jnp.float32)
        part_decay = jnp.dot(normed, decay_proj[section_index], preferred_element_type=jnp.float32)
        part_rate = jnp.dot(normed, rate_proj[section_index], preferred_element_type=jnp.float32)
        part_gate = jnp.dot(normed, gate_proj[section_index], preferred_element_type=jnp.float32)
        totals = lax.psum(squares, "dp")
        own_squares = lax.dynamic_slice_in_dim(totals, first_row, local_rows, 0)
        summed = (
            lax.psum_scatter(part_recept, "dp", scatter_dimension=0, tiled=True),
            lax.psum_scatter(part_key, "dp", scatter_dimension=0, tiled=True),
            lax.psum_scatter(part_value, "dp", scatter_dimension=0, tiled=True),
            lax.psum_scatter(part_decay, "dp", scatter_dimension=0, tiled=True),
            lax.psum_scatter(part_rate, "dp", scatter_dimension=0, tiled=True),
            lax.psum_scatter(part_gate, "dp", scatter_dimension=0, tiled=True),
        )
        inv_rms = lax.rsqrt(own_squares / D + norm_floor)

        def by_head(term):
            rounded = lax.optimization_barrier((inv_rms[:, None] * term).astype(jnp.bfloat16))
            return rounded.astype(jnp.float32).reshape(local_rows, local_heads, HEAD)

        decay_heads = by_head(summed[3]) + decay_base[section_index].reshape(1, local_heads, HEAD)
        updated, normal = recurrence(
            state[section_index].reshape(local_rows, local_heads, HEAD, HEAD),
            by_head(summed[0]),
            by_head(summed[1]),
            by_head(summed[2]),
            decay_heads,
            by_head(summed[4]),
        )
        finals.append(updated.reshape(local_rows, local_heads, HEAD * HEAD))
        gate_value = jax.nn.sigmoid(by_head(summed[5]).reshape(local_rows, local_heads * HEAD))
        mixed_heads = (
            normal.reshape(local_rows, local_heads * HEAD) * group_gain[section_index] * gate_value
        ).astype(jnp.bfloat16)
        weights_out = output_proj[section_index]

        def apply_out(piece, begin, weights_out=weights_out):
            return jnp.dot(piece, weights_out, preferred_element_type=jnp.float32)

        partial_out = apply_out(lax.all_gather(mixed_heads, "dp", axis=0, tiled=True), jnp.int32(0))
        total = lax.psum(partial_out, "tp")
        current = (floats + total).astype(jnp.bfloat16)
    return (current, jnp.stack(finals))


MESH = pl.DeviceIdType.MESH
NT = (((1,), (1,)), ((), ()))
PAIR = 2 * HEAD
VMEM_LIMIT = 57 * 1024 * 1024


class Grid:
    def __init__(self, tp):
        self.tp, self.nz, self.per = tp, tp // 4, tp // 2
        self.t, self.d = lax.axis_index("tp"), lax.axis_index("dp")
        self.z = self.t // 4
        x, y = lax.rem(self.t, 2), lax.rem(self.t // 2, 2)
        self.xp, self.yp = self.t + 1 - 2 * x, self.t + 2 - 4 * y
        self.xyp = self.xp + self.yp - self.t
        order = [sorted((k for k in range(self.nz) if k != z), key=lambda k: abs(k - z)) for z in range(self.nz)]
        self.line = []
        for k in range(self.nz - 1):
            level = order[0][k]
            for z in range(1, self.nz):
                level = jnp.where(self.z == z, order[z][k], level)
            self.line.append(level * 4 + lax.rem(self.t, 4))

    def over(self, base, chip):
        return base // 4 * 4 + lax.rem(chip, 4)

    def lots(self):
        return [self.t] + self.line


class Sender:
    def __init__(self, sem):
        self.sem = sem

    def put(self, src, dst, recv, t, d, when=None):
        op = pltpu.make_async_remote_copy(
            src_ref=src, dst_ref=dst, send_sem=self.sem, recv_sem=recv,
            device_id={"tp": t, "dp": d}, device_id_type=MESH,
        )
        if when is None:
            op.start()
        else:
            pl.when(when)(op.start)


def whole_of(ref, sem, grid):
    return pltpu.make_async_remote_copy(
        src_ref=ref, dst_ref=ref, send_sem=sem, recv_sem=sem,
        device_id={"tp": grid.xp, "dp": grid.d}, device_id_type=MESH,
    )


def landed(ref, recv, grid, when=None):
    op = whole_of(ref, recv, grid)
    if when is None:
        op.wait_recv()
    else:
        pl.when(when)(op.wait_recv)


def left(ref, send, grid, when=None):
    op = whole_of(ref, send, grid)
    if when is None:
        op.wait_send()
    else:
        pl.when(when)(op.wait_send)


def gather_heads(grid, buf, send, line, plane, meanwhile, beside):
    out = Sender(send)
    for chip in grid.line[::-1]:
        out.put(buf.at[grid.t], buf.at[grid.t], line.at[grid.z], chip, grid.d)
    for chip in (grid.xyp, grid.xp, grid.yp):
        out.put(buf.at[grid.t], buf.at[grid.t], plane, chip, grid.d)
    meanwhile()
    for block in grid.line:
        landed(buf.at[block], line.at[block // 4], grid)
        for chip in (grid.xyp, grid.xp, grid.yp):
            out.put(buf.at[block], buf.at[block], plane, chip, grid.d)
    beside()
    landed(buf.at[0 : 3 * grid.nz], plane, grid)
    left(buf.at[0 : 4 * grid.nz - 1], send, grid)


def gather_tiles(grid, buf, send, line, relayed, rest, use, after):
    out = Sender(send)

    def put(block, half, recv, chip):
        out.put(buf.at[block, half], buf.at[block, half], recv, chip, grid.d)

    def plane(block):
        level = block // 4
        put(block, 0, relayed.at[level, 0], grid.xp)
        put(block, 1, relayed.at[level, 1], grid.yp)
        put(block, 1, rest.at[level], grid.xp)
        put(block, 0, rest.at[level], grid.yp)

    def relay(lot):
        across, along, level = grid.over(lot, grid.xp), grid.over(lot, grid.yp), lot // 4
        landed(buf.at[across, 0], relayed.at[level, 0], grid)
        put(across, 0, rest.at[level], grid.yp)
        landed(buf.at[along, 1], relayed.at[level, 1], grid)
        put(along, 1, rest.at[level], grid.xp)

    for chip in grid.line:
        out.put(buf.at[grid.t], buf.at[grid.t], line.at[grid.z], chip, grid.d)
    plane(grid.t)
    last = grid.t
    for block in grid.line[:-1]:
        landed(buf.at[block], line.at[block // 4], grid)
        plane(block)
        relay(last)
        last = block
    block = grid.line[-1]
    landed(buf.at[block], line.at[block // 4], grid)
    for chip in (grid.xyp, grid.xp, grid.yp):
        out.put(buf.at[block], buf.at[block], rest.at[block // 4], chip, grid.d)
    relay(last)
    after()
    for k, lot in enumerate(grid.lots()):
        landed(buf.at[0 : 3 if k == grid.nz - 1 else 2], rest.at[lot // 4], grid)
        for block in (lot, grid.over(lot, grid.xp), grid.over(lot, grid.yp), grid.over(lot, grid.xyp)):
            use(block)

    def finish():
        left(buf.at[0 : 4 * grid.nz - 1], send, grid)

    return finish


def spread_result(grid, tile, final, send, line, relayed, rest):
    rows, lane = tile.shape[1], tile.shape[2]
    d, per, half_z = grid.d, grid.per, grid.nz // 2
    home = grid.t // per
    out, extra = Sender(send.at[0]), Sender(send.at[1])

    def place(block, r, half):
        at = pl.multiple_of((lax.rem(block, per) * 2 + half) * lane, lane)
        return final.at[pl.ds(pl.multiple_of(r * rows, rows), rows), pl.ds(at, lane)]

    def share(count):
        return final.at[pl.ds(0, count * rows // (2 * per))]

    def deep(block):
        return lax.rem(block // 4, half_z)

    def own(half, recv, chip, when=None):
        (out if when is None else extra).put(tile.at[half], place(grid.t, d, half), recv, chip, home, when)

    away = home != d
    level = deep(grid.t)
    for half in range(2):
        for chip in grid.line:
            own(half, line.at[level, d], chip)
    own(0, relayed.at[level, d, 0], grid.xp)
    own(1, relayed.at[level, d, 1], grid.yp)
    own(1, rest.at[0], grid.xp)
    own(0, rest.at[0], grid.yp)
    for half in range(2):
        own(half, rest.at[1], grid.t, away)

        @pl.when(home == d)
        def _(half=half):
            place(grid.t, d, half)[...] = tile[half]

    low = d * half_z
    lots = []
    for k in range(half_z):
        inside = low + lax.rem(grid.z - low + half_z + k, half_z)
        at = jnp.where(grid.z < low, low + k, jnp.where(grid.z >= low + half_z, low + half_z - 1 - k, inside))
        lots.append((at * 4 + lax.rem(grid.t, 4), at != grid.z))

    def put(block, r, half, recv, chip, far=None):
        (out if far is None else extra).put(place(block, r, half), place(block, r, half), recv, chip, d, far)

    def plane(lot, far):
        level = deep(lot)
        for r in range(2):
            landed(share(2), line.at[level, r], grid, far)
            put(lot, r, 0, relayed.at[level, r, 0], grid.xp, far)
            put(lot, r, 1, relayed.at[level, r, 1], grid.yp, far)
            put(lot, r, 1, rest.at[0], grid.xp, far)
            put(lot, r, 0, rest.at[0], grid.yp, far)

    def relay(lot):
        across, along, level = grid.over(lot, grid.xp), grid.over(lot, grid.yp), deep(lot)
        for r in range(2):
            landed(place(across, r, 0), relayed.at[level, r, 0], grid)
            put(across, r, 0, rest.at[0], grid.yp)
            landed(place(along, r, 1), relayed.at[level, r, 1], grid)
            put(along, r, 1, rest.at[0], grid.xp)

    def direct(lot):
        at = pl.multiple_of(lax.rem(lot, per) * 2 * lane, 2 * lane)
        for r in range(2):
            landed(share(2), line.at[deep(lot), r], grid)
            ref = final.at[pl.ds(r * rows, rows), pl.ds(at, 2 * lane)]
            for chip in (grid.xyp, grid.xp, grid.yp):
                out.put(ref, ref, rest.at[0], chip, d)

    for lot, far in lots[:-1]:
        plane(lot, far)
    direct(lots[-1][0])
    for lot, far in lots[:-1]:
        relay(lot)
    landed(share(8 * half_z + 4), rest.at[0], grid)
    landed(share(2), rest.at[1], grid, home_is(grid))
    left(share(2 * (grid.nz - 1) + 4 * half_z + 12), send.at[0], grid)
    left(share(2), send.at[1], grid, away)
    for lot, far in lots[:-1]:
        left(share(8), send.at[1], grid, far)


def home_is(grid):
    return grid.t // grid.per == grid.d


def iota(shape, axis):
    return lax.broadcasted_iota(jnp.int32, shape, axis)


def update_state(proj, base, ggain, layer, old, new, terms, reads, seqs):
    mine = proj.shape[0]
    lines = old.shape[1] // mine

    def piece(i):
        return proj[:, i * HEAD : (i + 1) * HEAD].astype(jnp.float32)

    recept, key, value, decay, rate = [piece(i) for i in range(5)]
    scale = lax.rsqrt(jnp.sum(key * key, axis=-1, keepdims=True) + 1.0)
    forget = jnp.exp(-jnp.exp(-jax.nn.softplus(-(decay + base[layer : layer + 1, :])) - 0.5))
    learned = key * jax.nn.sigmoid(rate)
    for i, term in enumerate((key * (-scale * scale), forget, learned, recept, value)):
        terms[i] = jnp.concatenate([term, term], axis=-1)

    lane, col = iota((PAIR, PAIR), 0), iota((PAIR, PAIR), 1)
    same = (lane // HEAD == col // HEAD).astype(jnp.bfloat16)
    odd = ((lane < HEAD) & (lane % 2 == col // HEAD)).astype(jnp.bfloat16)
    turn = (lane // HEAD == col % 2).astype(jnp.bfloat16)
    both = jnp.concatenate([same, odd], axis=0)
    mask = (iota((lines, PAIR), 1) % HEAD) // 2 == iota((lines, PAIR), 0)

    def step(i, carry):
        begin = pl.multiple_of(i * seqs, seqs)
        first = pl.multiple_of(i * seqs * lines, seqs * lines)

        def spread(k):
            return jnp.broadcast_to(terms[k, pl.ds(begin, seqs), :][:, None, :], (seqs, lines, PAIR))

        state = old[layer, pl.ds(first, seqs * lines), :].reshape(seqs, lines, PAIR)
        product = (state * spread(0)).astype(jnp.bfloat16).reshape(seqs * lines, PAIR)
        chosen = jnp.where(mask[None], spread(4), 0.0).astype(jnp.bfloat16).reshape(seqs * lines, PAIR)
        rank = jnp.dot(jnp.concatenate([product, chosen], axis=1), both, preferred_element_type=jnp.float32)
        updated = state * spread(1) + rank.reshape(seqs, lines, PAIR) * spread(2)
        new[layer, pl.ds(first, seqs * lines), :] = updated.reshape(seqs * lines, PAIR)
        weighed = (updated * spread(3)).astype(jnp.bfloat16).reshape(seqs * lines, PAIR)
        read = jnp.dot(weighed, turn, preferred_element_type=jnp.float32).reshape(seqs, lines, PAIR)
        reads[pl.ds(begin, seqs), :] = jnp.sum(jnp.where(mask[None], read, 0.0), axis=1)
        return carry

    lax.fori_loop(0, mine // seqs, step, 0)
    read = reads[:, :HEAD]
    centre = read - jnp.mean(read, axis=-1, keepdims=True)
    normal = centre * lax.rsqrt(jnp.mean(centre * centre, axis=-1, keepdims=True) + group_floor)
    return (normal * ggain[layer : layer + 1, :] * jax.nn.sigmoid(piece(5))).astype(jnp.bfloat16)


def whole_kernel(
    tp, tok, gain, wr, wk, wv, wd, wa, wg, wo, base_in, ggain_in, state, final, new,
    tokv, w0, w1, gains, part, inbox, acc, near, outw, we, mg, xg, tile, old, terms, reads, proj, base, ggain,
    load, pair_send, pair_recv, a2a_send, a2a_recv, on_send, on_recv, m_send, m_line, m_plane,
    x_send, x_line, x_relayed, x_rest, f_send, f_line, f_relayed, f_rest,
):
    grid = Grid(tp)
    t, d, per = grid.t, grid.d, grid.per
    rows, feats = tok.shape
    mine = rows // 2
    cols = near.shape[1]
    width = 6 * HEAD
    weights = (wr, wk, wv, wd, wa, wg)
    here, there = pl.multiple_of(d * mine, mine), pl.multiple_of((1 - d) * mine, mine)

    def copy(src, dst, number):
        return pltpu.make_async_copy(src, dst, load.at[number])

    get_there = copy(tok.at[pl.ds(there, mine)], tokv.at[pl.ds(there, mine)], 0)
    get_here = copy(tok.at[pl.ds(here, mine)], tokv.at[pl.ds(here, mine)], 1)
    get_gain = copy(gain, gains.at[d], 2)
    get_base, get_ggain = copy(base_in, base, 3), copy(ggain_in, ggain, 4)
    get_w0 = [copy(w.at[0], w0.at[pl.ds(i * HEAD, HEAD)], 5) for i, w in enumerate(weights)]
    get_w1 = [copy(w.at[1], w1.at[d, pl.ds(i * HEAD, HEAD)], 6) for i, w in enumerate(weights)]
    get_state = [copy(state.at[k], old.at[k], 7 + k) for k in range(LAYERS)]
    for op in [get_there, get_gain] + get_w0 + [get_here, get_base, get_ggain]:
        op.start()

    barrier = pltpu.get_barrier_semaphore()
    for k in range(1, tp):
        for core in range(2):
            pl.semaphore_signal(barrier, inc=1, device_id={"tp": lax.rem(t + k, tp), "dp": core}, device_id_type=MESH)
    pl.semaphore_signal(barrier, inc=1, device_id={"tp": t, "dp": 1 - d}, device_id_type=MESH)
    for op in [get_state[0]] + get_w1 + [get_state[1]]:
        op.start()

    def project(begin):
        floats = tokv[pl.ds(begin, mine), :].astype(jnp.float32)
        part[pl.ds(begin, mine), width:] = jnp.broadcast_to(jnp.sum(floats * floats, axis=1, keepdims=True), (mine, PAIR))
        normed = (floats * gains[d, 0:1, :]).astype(jnp.bfloat16)
        part[pl.ds(begin, mine), 0:width] = lax.dot_general(normed, w0[...], NT, preferred_element_type=jnp.float32)

    get_there.wait()
    get_gain.wait()
    copy(w0, w0, 5).wait()
    project(there)
    get_here.wait()
    project(here)
    pl.semaphore_wait(barrier, 2 * tp - 1)

    def to_partner(number, src, dst):
        Sender(pair_send.at[number]).put(src, dst, pair_recv.at[number], t, 1 - d)

    slot = lax.rem(t, per)
    slot_cols = pl.ds(pl.multiple_of(slot * cols, cols), cols)
    to_partner(0, part.at[pl.ds(there, mine)], inbox)
    to_partner(1, tokv.at[pl.ds(there, mine), slot_cols], near)
    to_partner(2, gains.at[d], gains.at[d])

    home = home_is(grid)

    def spread_weights(layer):
        for c in range(per):
            block = wo.at[layer, :, pl.ds(c * cols, cols)]
            target = d * per + c
            Sender(a2a_send.at[layer]).put(block, outw.at[layer, t], a2a_recv.at[layer], target, d, when=target != t)

            @pl.when(target == t)
            def _(block=block):
                pltpu.make_async_copy(block, outw.at[layer, t], a2a_recv.at[layer]).start()

    def weights_left(layer):
        left(outw.at[layer, 0:per], a2a_send.at[layer], grid, jnp.logical_not(home))
        left(outw.at[layer, 0 : per - 1], a2a_send.at[layer], grid, home)
        left(outw.at[layer], on_send.at[layer], grid, home)

    spread_weights(0)
    for i, w in enumerate(weights):
        to_partner(3, w.at[1], w1.at[d, pl.ds(i * HEAD, HEAD)])

    get_base.wait()
    get_ggain.wait()
    landed(inbox, pair_recv.at[0], grid)
    total = part[pl.ds(here, mine), :] + inbox[...]
    inv = lax.rsqrt(total[:, width : width + 1] / (feats * 2) + norm_floor)
    proj[...] = (inv * total[:, :width]).astype(jnp.bfloat16)

    landed(near, pair_recv.at[1], grid)
    own = tokv[pl.ds(here, mine), slot_cols].astype(jnp.float32)
    ours = home.astype(jnp.float32)
    current = own * ours + near[...].astype(jnp.float32) * (1.0 - ours)

    def forward_weights(layer):
        landed(outw.at[layer], a2a_recv.at[layer], grid, home)
        Sender(on_send.at[layer]).put(outw.at[layer], outw.at[layer], on_recv.at[layer], t, 1 - d, when=home)
        landed(outw.at[layer], on_recv.at[layer], grid, jnp.logical_not(home))

    def project_out(layer, mixed, current):
        half = mine // 2
        mg[layer, t] = jnp.concatenate([mixed[0:half, :], mixed[half:mine, :]], axis=1)

        def meanwhile():
            if layer + 1 < LAYERS:
                pass

        def beside():
            forward_weights(layer)
            zero = jnp.zeros((HEAD, cols), we.dtype)
            for k in range(tp):
                block = outw[layer, k]
                top, bottom = pl.ds(k * PAIR, HEAD), pl.ds(k * PAIR + HEAD, HEAD)
                we[top, 0:cols] = block
                we[top, cols : 2 * cols] = zero
                we[bottom, 0:cols] = zero
                we[bottom, cols : 2 * cols] = block

        gather_heads(grid, mg.at[layer], m_send.at[layer], m_line.at[layer], m_plane.at[layer], meanwhile, beside)
        packed = jnp.concatenate([mg[layer, j] for j in range(tp)], axis=1)
        out = jnp.dot(packed, we[...], preferred_element_type=jnp.float32)
        out = jnp.concatenate([out[:, :cols], out[:, cols:]], axis=0)
        return (current + out).astype(jnp.bfloat16)

    seqs = min(mine, 16)
    get_state[0].wait()
    mixed = update_state(proj, base, ggain, 0, old, new, terms, reads, seqs)
    stream = project_out(0, mixed, current)

    lane = cols // 2
    for k in range(2):
        xg[t, k] = stream[:, k * lane : (k + 1) * lane]
    copy(w1.at[d], w1.at[d], 6).wait()
    landed(w1.at[1 - d], pair_recv.at[3], grid)
    landed(gains.at[1 - d], pair_recv.at[2], grid)
    acc[...] = jnp.zeros(acc.shape, jnp.float32)

    def use(block):
        half, at = block // per, pl.multiple_of(lax.rem(block, per) * cols, cols)
        floats = jnp.concatenate([xg[block, k] for k in range(2)], axis=1).astype(jnp.float32)
        normed = (floats * gains[half, 1:2, pl.ds(at, cols)]).astype(jnp.bfloat16)
        weight = w1[half, :, pl.ds(at, cols)]
        acc[:, 0:width] += lax.dot_general(normed, weight, NT, preferred_element_type=jnp.float32)
        squares = floats * floats
        for k in range(cols // PAIR):
            acc[:, width:] += squares[:, k * PAIR : (k + 1) * PAIR]

    tiles_left = gather_tiles(grid, xg, x_send, x_line, x_relayed, x_rest, use, lambda: spread_weights(1))
    inv = lax.rsqrt(jnp.sum(acc[:, width:], axis=1, keepdims=True) / (feats * 2) + norm_floor)
    proj[...] = (inv * acc[:, 0:width]).astype(jnp.bfloat16)

    get_state[1].wait()
    mixed = update_state(proj, base, ggain, 1, old, new, terms, reads, seqs)
    stream = project_out(1, mixed, stream.astype(jnp.float32))
    for k in range(2):
        tile[k] = stream[:, k * lane : (k + 1) * lane]
    spread_result(grid, tile, final, f_send, f_line, f_relayed, f_rest)

    tiles_left()
    left(part.at[pl.ds(there, mine)], pair_send.at[0], grid)
    left(near, pair_send.at[1], grid)
    left(gains.at[d], pair_send.at[2], grid)
    left(w1.at[d], pair_send.at[3], grid)
    for layer in range(LAYERS):
        weights_left(layer)


def store_kernel(final, new, final_out, new_out, sems):
    ops = [pltpu.make_async_copy(new, new_out, sems.at[0]), pltpu.make_async_copy(final, final_out, sems.at[1])]
    for op in ops:
        op.start()
    for op in ops:
        op.wait()


def fast(tp, tokens, norm_gain, projections, decay_base, group_gain, output_proj, state):
    rows, feats = tokens.shape
    mine, per = rows // 2, tp // 2
    cols = feats // per
    width = 6 * HEAD
    lines = HEAD * HEAD // PAIR
    bf, f32 = jnp.bfloat16, jnp.float32
    shape, vmem, dma = jax.ShapeDtypeStruct, pltpu.VMEM, pltpu.SemaphoreType.DMA
    inside, anywhere = pl.BlockSpec(memory_space=pltpu.VMEM), pl.BlockSpec(memory_space=pl.ANY)
    turned = [jnp.swapaxes(w, 1, 2) for w in projections]
    flat = state.reshape(LAYERS, mine * lines, PAIR)
    outs = (shape((rows, feats), bf), shape(flat.shape, f32))
    final, new = pl.pallas_call(
        functools.partial(whole_kernel, tp),
        out_shape=(vmem((rows, feats), bf), vmem(flat.shape, f32)),
        in_specs=[pl.BlockSpec(memory_space=pltpu.HBM)] * 12,
        out_specs=(inside, inside),
        scratch_shapes=[
            vmem((rows, feats), bf), vmem((width, feats), bf), vmem((2, width, feats), bf), vmem((2, LAYERS, feats), f32),
            vmem((rows, width + PAIR), f32), vmem((mine, width + PAIR), f32), vmem((mine, width + PAIR), f32),
            vmem((mine, cols), bf),
            vmem((LAYERS, tp, HEAD, cols), bf), vmem((tp * PAIR, 2 * cols), bf), vmem((LAYERS, tp, mine // 2, PAIR), bf),
            vmem((tp, 2, mine, cols // 2), bf), vmem((2, mine, cols // 2), bf), vmem(flat.shape, f32),
            vmem((5, mine, PAIR), f32), vmem((mine, PAIR), f32), vmem((mine, width), bf),
            vmem((LAYERS, HEAD), f32), vmem((LAYERS, HEAD), f32),
            dma((9,)), dma((4,)), dma((4,)), dma((LAYERS,)), dma((LAYERS,)), dma((LAYERS,)), dma((LAYERS,)),
            dma((LAYERS,)), dma((LAYERS, tp // 4)), dma((LAYERS,)),
            dma, dma((tp // 4,)), dma((tp // 4, 2)), dma((tp // 4,)),
            dma((2,)), dma((tp // 8, 2)), dma((tp // 8, 2, 2)), dma((2,)),
        ],
        compiler_params=pltpu.CompilerParams(collective_id=0, has_side_effects=True, vmem_limit_bytes=VMEM_LIMIT),
        name="whole",
    )(tokens, norm_gain, *turned, output_proj, decay_base, group_gain, flat)
    final, new = pl.pallas_call(
        store_kernel,
        out_shape=outs,
        in_specs=[inside, inside],
        out_specs=(anywhere, anywhere),
        scratch_shapes=[dma((2,))],
        compiler_params=pltpu.CompilerParams(vmem_limit_bytes=1024 * 1024),
        name="store",
    )(final, new)
    return (final, new.reshape(state.shape))


def step(tp, dp, tokens, norm_gain, *rest):
    projections, (decay_base, group_gain, output_proj, state) = rest[:6], rest[6:]
    rows, feats = tokens.shape
    fits = dp == 2 and tp % 16 == 0 and state.shape[2] == 1 and state.shape[1] % 64 == 0 and (feats * dp // tp) % 256 == 0
    if fits:
        return fast(tp, tokens, norm_gain, projections, decay_base, group_gain, output_proj, state)
    return shards(tokens, norm_gain, *rest)


def solution(mesh):
    return jax.shard_map(
        functools.partial(step, mesh.shape["tp"], mesh.shape["dp"]),
        mesh=mesh,
        in_specs=(
            P(None, "dp"),
            P(None, "dp"),
            P(None, "dp", "tp"),
            P(None, "dp", "tp"),
            P(None, "dp", "tp"),
            P(None, "dp", "tp"),
            P(None, "dp", "tp"),
            P(None, "dp", "tp"),
            P(None, "tp"),
            P(None, "tp"),
            P(None, "tp", "dp"),
            P(None, "dp", "tp", None),
        ),
        out_specs=(P(None, "dp"), P(None, "dp", "tp", None)),
        check_vma=False,
    )
```

```python
import functools
import math

import jax
import jax.numpy as jnp
from jax import lax
from jax.experimental import pallas as pl
from jax.experimental.pallas import tpu as pltpu
from jax.sharding import PartitionSpec as P

D = 4096
HEAD = 64
LAYERS = 2


norm_floor = 0.1
group_floor = 0.5


def recurrence(state_block, recept_heads, key_heads, value_heads, decay_heads, rate_heads):
    log_rate = -jax.nn.softplus(-decay_heads) - 0.5
    forget = jnp.exp(-jnp.exp(log_rate))
    learn_rate = jax.nn.sigmoid(rate_heads)
    unit_key = key_heads * lax.rsqrt(jnp.sum(key_heads * key_heads, axis=-1, keepdims=True) + 1.0)
    scaled = key_heads * learn_rate
    removed = jnp.einsum("bhvk,bhk->bhv", state_block, -unit_key, precision=lax.Precision.HIGHEST)
    updated = (
        state_block * forget[:, :, None, :]
        + removed[..., None] * (unit_key * learn_rate)[:, :, None, :]
        + value_heads[..., None] * scaled[:, :, None, :]
    )
    read_out = jnp.einsum("bhvk,bhk->bhv", updated, recept_heads, precision=lax.Precision.HIGHEST)
    centre = read_out - jnp.mean(read_out, axis=-1, keepdims=True)
    normal = centre * lax.rsqrt(jnp.mean(centre * centre, axis=-1, keepdims=True) + group_floor)
    return (updated, normal)


def shards(
    tokens,
    norm_gain,
    receptance,
    key_proj,
    value_proj,
    decay_proj,
    rate_proj,
    gate_proj,
    decay_base,
    group_gain,
    output_proj,
    state,
):
    local_rows = state.shape[1]
    first_row = lax.axis_index("dp") * local_rows
    local_heads = state.shape[2]
    current = tokens
    finals = []
    for section_index in range(LAYERS):
        floats = current.astype(jnp.float32)
        squares = jnp.sum(floats * floats, axis=1)
        normed = (floats * norm_gain[section_index]).astype(jnp.bfloat16)
        part_recept = jnp.dot(normed, receptance[section_index], preferred_element_type=jnp.float32)
        part_key = jnp.dot(normed, key_proj[section_index], preferred_element_type=jnp.float32)
        part_value = jnp.dot(normed, value_proj[section_index], preferred_element_type=jnp.float32)
        part_decay = jnp.dot(normed, decay_proj[section_index], preferred_element_type=jnp.float32)
        part_rate = jnp.dot(normed, rate_proj[section_index], preferred_element_type=jnp.float32)
        part_gate = jnp.dot(normed, gate_proj[section_index], preferred_element_type=jnp.float32)
        totals = lax.psum(squares, "dp")
        own_squares = lax.dynamic_slice_in_dim(totals, first_row, local_rows, 0)
        summed = (
            lax.psum_scatter(part_recept, "dp", scatter_dimension=0, tiled=True),
            lax.psum_scatter(part_key, "dp", scatter_dimension=0, tiled=True),
            lax.psum_scatter(part_value, "dp", scatter_dimension=0, tiled=True),
            lax.psum_scatter(part_decay, "dp", scatter_dimension=0, tiled=True),
            lax.psum_scatter(part_rate, "dp", scatter_dimension=0, tiled=True),
            lax.psum_scatter(part_gate, "dp", scatter_dimension=0, tiled=True),
        )
        inv_rms = lax.rsqrt(own_squares / D + norm_floor)

        def by_head(term):
            rounded = lax.optimization_barrier((inv_rms[:, None] * term).astype(jnp.bfloat16))
            return rounded.astype(jnp.float32).reshape(local_rows, local_heads, HEAD)

        decay_heads = by_head(summed[3]) + decay_base[section_index].reshape(1, local_heads, HEAD)
        updated, normal = recurrence(
            state[section_index].reshape(local_rows, local_heads, HEAD, HEAD),
            by_head(summed[0]),
            by_head(summed[1]),
            by_head(summed[2]),
            decay_heads,
            by_head(summed[4]),
        )
        finals.append(updated.reshape(local_rows, local_heads, HEAD * HEAD))
        gate_value = jax.nn.sigmoid(by_head(summed[5]).reshape(local_rows, local_heads * HEAD))
        mixed_heads = (
            normal.reshape(local_rows, local_heads * HEAD) * group_gain[section_index] * gate_value
        ).astype(jnp.bfloat16)
        weights_out = output_proj[section_index]

        def apply_out(piece, begin, weights_out=weights_out):
            return jnp.dot(piece, weights_out, preferred_element_type=jnp.float32)

        partial_out = apply_out(lax.all_gather(mixed_heads, "dp", axis=0, tiled=True), jnp.int32(0))
        total = lax.psum(partial_out, "tp")
        current = (floats + total).astype(jnp.bfloat16)
    return (current, jnp.stack(finals))


MESH = pl.DeviceIdType.MESH
NT = (((1,), (1,)), ((), ()))
PAIR = 2 * HEAD
VMEM_LIMIT = 57 * 1024 * 1024


class Grid:
    def __init__(self, tp):
        self.tp, self.nz, self.per = tp, tp // 4, tp // 2
        self.t, self.d = lax.axis_index("tp"), lax.axis_index("dp")
        self.z = self.t // 4
        x, y = lax.rem(self.t, 2), lax.rem(self.t // 2, 2)
        self.xp, self.yp = self.t + 1 - 2 * x, self.t + 2 - 4 * y
        self.xyp = self.xp + self.yp - self.t
        order = [sorted((k for k in range(self.nz) if k != z), key=lambda k: abs(k - z)) for z in range(self.nz)]
        self.line = []
        for k in range(self.nz - 1):
            level = order[0][k]
            for z in range(1, self.nz):
                level = jnp.where(self.z == z, order[z][k], level)
            self.line.append(level * 4 + lax.rem(self.t, 4))

    def over(self, base, chip):
        return base // 4 * 4 + lax.rem(chip, 4)

    def lots(self):
        return [self.t] + self.line


class Sender:
    def __init__(self, sem):
        self.sem = sem

    def put(self, src, dst, recv, t, d, when=None):
        op = pltpu.make_async_remote_copy(
            src_ref=src, dst_ref=dst, send_sem=self.sem, recv_sem=recv,
            device_id={"tp": t, "dp": d}, device_id_type=MESH,
        )
        if when is None:
            op.start()
        else:
            pl.when(when)(op.start)


def whole_of(ref, sem, grid):
    return pltpu.make_async_remote_copy(
        src_ref=ref, dst_ref=ref, send_sem=sem, recv_sem=sem,
        device_id={"tp": grid.xp, "dp": grid.d}, device_id_type=MESH,
    )


def landed(ref, recv, grid, when=None):
    op = whole_of(ref, recv, grid)
    if when is None:
        op.wait_recv()
    else:
        pl.when(when)(op.wait_recv)


def left(ref, send, grid, when=None):
    op = whole_of(ref, send, grid)
    if when is None:
        op.wait_send()
    else:
        pl.when(when)(op.wait_send)


def gather_heads(grid, buf, send, line, plane, meanwhile, beside):
    out = Sender(send)
    for chip in grid.line[::-1]:
        out.put(buf.at[grid.t], buf.at[grid.t], line.at[grid.z], chip, grid.d)
    for chip in (grid.xyp, grid.xp, grid.yp):
        out.put(buf.at[grid.t], buf.at[grid.t], plane, chip, grid.d)
    meanwhile()
    for block in grid.line:
        landed(buf.at[block], line.at[block // 4], grid)
        for chip in (grid.xyp, grid.xp, grid.yp):
            out.put(buf.at[block], buf.at[block], plane, chip, grid.d)
    beside()
    landed(buf.at[0 : 3 * grid.nz], plane, grid)
    left(buf.at[0 : 4 * grid.nz - 1], send, grid)


def gather_tiles(grid, buf, send, line, relayed, rest, use, after):
    out = Sender(send)

    def put(block, half, recv, chip):
        out.put(buf.at[block, half], buf.at[block, half], recv, chip, grid.d)

    def plane(block):
        level = block // 4
        put(block, 0, relayed.at[level, 0], grid.xp)
        put(block, 1, relayed.at[level, 1], grid.yp)
        put(block, 1, rest.at[level], grid.xp)
        put(block, 0, rest.at[level], grid.yp)

    def relay(lot):
        across, along, level = grid.over(lot, grid.xp), grid.over(lot, grid.yp), lot // 4
        landed(buf.at[across, 0], relayed.at[level, 0], grid)
        put(across, 0, rest.at[level], grid.yp)
        landed(buf.at[along, 1], relayed.at[level, 1], grid)
        put(along, 1, rest.at[level], grid.xp)

    for chip in grid.line:
        out.put(buf.at[grid.t], buf.at[grid.t], line.at[grid.z], chip, grid.d)
    plane(grid.t)
    last = grid.t
    for block in grid.line[:-1]:
        landed(buf.at[block], line.at[block // 4], grid)
        plane(block)
        relay(last)
        last = block
    block = grid.line[-1]
    landed(buf.at[block], line.at[block // 4], grid)
    for chip in (grid.xyp, grid.xp, grid.yp):
        out.put(buf.at[block], buf.at[block], rest.at[block // 4], chip, grid.d)
    relay(last)
    after()
    for k, lot in enumerate(grid.lots()):
        landed(buf.at[0 : 3 if k == grid.nz - 1 else 2], rest.at[lot // 4], grid)
        for block in (lot, grid.over(lot, grid.xp), grid.over(lot, grid.yp), grid.over(lot, grid.xyp)):
            use(block)

    def finish():
        left(buf.at[0 : 4 * grid.nz - 1], send, grid)

    return finish


def spread_result(grid, tile, final, send, line, relayed, rest):
    rows, lane = tile.shape[1], tile.shape[2]
    d, per, half_z = grid.d, grid.per, grid.nz // 2
    home = grid.t // per
    out, extra = Sender(send.at[0]), Sender(send.at[1])

    def place(block, r, half):
        at = pl.multiple_of((lax.rem(block, per) * 2 + half) * lane, lane)
        return final.at[pl.ds(pl.multiple_of(r * rows, rows), rows), pl.ds(at, lane)]

    def share(count):
        return final.at[pl.ds(0, count * rows // (2 * per))]

    def deep(block):
        return lax.rem(block // 4, half_z)

    def own(half, recv, chip, when=None):
        (out if when is None else extra).put(tile.at[half], place(grid.t, d, half), recv, chip, home, when)

    away = home != d
    level = deep(grid.t)
    for half in range(2):
        for chip in grid.line:
            own(half, line.at[level, d], chip)
    own(0, relayed.at[level, d, 0], grid.xp)
    own(1, relayed.at[level, d, 1], grid.yp)
    own(1, rest.at[0], grid.xp)
    own(0, rest.at[0], grid.yp)
    for half in range(2):
        own(half, rest.at[1], grid.t, away)

        @pl.when(home == d)
        def _(half=half):
            place(grid.t, d, half)[...] = tile[half]

    low = d * half_z
    lots = []
    for k in range(half_z):
        inside = low + lax.rem(grid.z - low + half_z + k, half_z)
        at = jnp.where(grid.z < low, low + k, jnp.where(grid.z >= low + half_z, low + half_z - 1 - k, inside))
        lots.append((at * 4 + lax.rem(grid.t, 4), at != grid.z))

    def put(block, r, half, recv, chip, far=None):
        (out if far is None else extra).put(place(block, r, half), place(block, r, half), recv, chip, d, far)

    def plane(lot, far):
        level = deep(lot)
        for r in range(2):
            landed(share(2), line.at[level, r], grid, far)
            put(lot, r, 0, relayed.at[level, r, 0], grid.xp, far)
            put(lot, r, 1, relayed.at[level, r, 1], grid.yp, far)
            put(lot, r, 1, rest.at[0], grid.xp, far)
            put(lot, r, 0, rest.at[0], grid.yp, far)

    def relay(lot):
        across, along, level = grid.over(lot, grid.xp), grid.over(lot, grid.yp), deep(lot)
        for r in range(2):
            landed(place(across, r, 0), relayed.at[level, r, 0], grid)
            put(across, r, 0, rest.at[0], grid.yp)
            landed(place(along, r, 1), relayed.at[level, r, 1], grid)
            put(along, r, 1, rest.at[0], grid.xp)

    def direct(lot):
        at = pl.multiple_of(lax.rem(lot, per) * 2 * lane, 2 * lane)
        for r in range(2):
            landed(share(2), line.at[deep(lot), r], grid)
            ref = final.at[pl.ds(r * rows, rows), pl.ds(at, 2 * lane)]
            for chip in (grid.xyp, grid.xp, grid.yp):
                out.put(ref, ref, rest.at[0], chip, d)

    for lot, far in lots[:-1]:
        plane(lot, far)
    direct(lots[-1][0])
    for lot, far in lots[:-1]:
        relay(lot)
    landed(share(8 * half_z + 4), rest.at[0], grid)
    landed(share(2), rest.at[1], grid, home_is(grid))
    left(share(2 * (grid.nz - 1) + 4 * half_z + 12), send.at[0], grid)
    left(share(2), send.at[1], grid, away)
    for lot, far in lots[:-1]:
        left(share(8), send.at[1], grid, far)


def home_is(grid):
    return grid.t // grid.per == grid.d


def iota(shape, axis):
    return lax.broadcasted_iota(jnp.int32, shape, axis)


def update_state(proj, base, ggain, layer, old, new, terms, reads, doubled, seqs):
    mine = proj.shape[0]
    lines = old.shape[1] // mine
    wide = jnp.dot(proj[...], doubled[...], preferred_element_type=jnp.float32)

    def piece(i):
        return wide[:, i * PAIR : (i + 1) * PAIR]

    def twice(row):
        return jnp.concatenate([row, row], axis=-1)

    recept, key, value, decay, rate, gate = [piece(i) for i in range(6)]
    scale = lax.rsqrt(jnp.sum(key * key, axis=-1, keepdims=True) * 0.5 + 1.0)
    forget = jnp.exp(-math.exp(-0.5) * jax.nn.sigmoid(decay + twice(base[layer : layer + 1, :])))
    learned = key * jax.nn.sigmoid(rate)
    for i, term in enumerate((key * (-scale * scale), forget, learned, recept, value)):
        terms[i] = term

    lane, col = iota((PAIR, PAIR), 0), iota((PAIR, PAIR), 1)
    same = (lane // HEAD == col // HEAD).astype(jnp.bfloat16)
    odd = ((lane < HEAD) & (lane % 2 == col // HEAD)).astype(jnp.bfloat16)
    turn = (lane // HEAD == col % 2).astype(jnp.bfloat16)
    both = jnp.concatenate([same, odd], axis=0)
    mask = (iota((lines, PAIR), 1) % HEAD) // 2 == iota((lines, PAIR), 0)

    def step(i, carry):
        begin = pl.multiple_of(i * seqs, seqs)
        first = pl.multiple_of(i * seqs * lines, seqs * lines)

        def spread(k):
            return jnp.broadcast_to(terms[k, pl.ds(begin, seqs), :][:, None, :], (seqs, lines, PAIR))

        state = old[layer, pl.ds(first, seqs * lines), :].reshape(seqs, lines, PAIR)
        product = (state * spread(0)).astype(jnp.bfloat16).reshape(seqs * lines, PAIR)
        chosen = jnp.where(mask[None], spread(4), 0.0).astype(jnp.bfloat16).reshape(seqs * lines, PAIR)
        rank = jnp.dot(jnp.concatenate([product, chosen], axis=1), both, preferred_element_type=jnp.float32)
        updated = state * spread(1) + rank.reshape(seqs, lines, PAIR) * spread(2)
        new[layer, pl.ds(first, seqs * lines), :] = updated.reshape(seqs * lines, PAIR)
        weighed = (updated * spread(3)).astype(jnp.bfloat16).reshape(seqs * lines, PAIR)
        read = jnp.dot(weighed, turn, preferred_element_type=jnp.float32).reshape(seqs, lines, PAIR)
        reads[pl.ds(begin, seqs), :] = jnp.sum(jnp.where(mask[None], read, 0.0), axis=1)
        return carry

    lax.fori_loop(0, mine // seqs, step, 0)
    read = reads[...]
    centre = read - jnp.mean(read, axis=-1, keepdims=True)
    normal = centre * lax.rsqrt(jnp.mean(centre * centre, axis=-1, keepdims=True) + group_floor)
    mixed = normal * twice(ggain[layer : layer + 1, :]) * jax.nn.sigmoid(gate)
    first = iota((mine // 2, PAIR), 1) < HEAD
    return jnp.where(first, mixed[0 : mine // 2], mixed[mine // 2 : mine]).astype(jnp.bfloat16)


def whole_kernel(
    tp, tok, gain, wr, wk, wv, wd, wa, wg, wo, base_in, ggain_in, state, final, new,
    tokv, w0, w1, gains, part, inbox, acc, near, outw, wov, hub, we, mg, xg, tile, old, terms, reads, doubled, proj, base, ggain,
    load, pair_send, pair_recv, hub_send, hub_recv, a2a_send, a2a_recv, on_send, on_recv, m_send, m_line, m_plane,
    x_send, x_line, x_relayed, x_rest, f_send, f_line, f_relayed, f_rest,
):
    grid = Grid(tp)
    t, d, per = grid.t, grid.d, grid.per
    rows, feats = tok.shape
    mine = rows // 2
    cols = near.shape[1]
    width = 6 * HEAD
    weights = (wr, wk, wv, wd, wa, wg)
    here, there = pl.multiple_of(d * mine, mine), pl.multiple_of((1 - d) * mine, mine)

    def copy(src, dst, number):
        return pltpu.make_async_copy(src, dst, load.at[number])

    get_there = copy(tok.at[pl.ds(there, mine)], tokv.at[pl.ds(there, mine)], 0)
    get_here = copy(tok.at[pl.ds(here, mine)], tokv.at[pl.ds(here, mine)], 1)
    get_gain = copy(gain, gains.at[d], 2)
    get_base, get_ggain = copy(base_in, base, 3), copy(ggain_in, ggain, 4)
    get_w0 = [copy(w.at[0], w0.at[pl.ds(i * HEAD, HEAD)], 5) for i, w in enumerate(weights)]
    get_w1 = [copy(w.at[1], w1.at[d, pl.ds(i * HEAD, HEAD)], 6) for i, w in enumerate(weights)]
    get_wo = copy(wo.at[0], wov, 9)
    get_state = [copy(state.at[k], old.at[k], 7 + k) for k in range(LAYERS)]
    for op in [get_there, get_gain] + get_w0 + [get_here, get_base, get_ggain]:
        op.start()

    barrier = pltpu.get_barrier_semaphore()
    for k in range(1, tp):
        for core in range(2):
            pl.semaphore_signal(barrier, inc=1, device_id={"tp": lax.rem(t + k, tp), "dp": core}, device_id_type=MESH)
    pl.semaphore_signal(barrier, inc=1, device_id={"tp": t, "dp": 1 - d}, device_id_type=MESH)
    for op in [get_wo, get_state[0]] + get_w1 + [get_state[1]]:
        op.start()
    source, column = iota((width, 2 * width), 0), iota((width, 2 * width), 1)
    wanted = column // PAIR * HEAD + column % HEAD
    doubled[...] = (source == wanted).astype(jnp.bfloat16)

    def project(begin):
        floats = tokv[pl.ds(begin, mine), :].astype(jnp.float32)
        part[pl.ds(begin, mine), width:] = jnp.broadcast_to(jnp.sum(floats * floats, axis=1, keepdims=True), (mine, PAIR))
        normed = (floats * gains[d, 0:1, :]).astype(jnp.bfloat16)
        part[pl.ds(begin, mine), 0:width] = lax.dot_general(normed, w0[...], NT, preferred_element_type=jnp.float32)

    get_there.wait()
    get_gain.wait()
    copy(w0, w0, 5).wait()
    project(there)
    get_here.wait()
    project(here)
    pl.semaphore_wait(barrier, 2 * tp - 1)

    def to_partner(number, src, dst):
        Sender(pair_send.at[number]).put(src, dst, pair_recv.at[number], t, 1 - d)

    slot = lax.rem(t, per)
    slot_cols = pl.ds(pl.multiple_of(slot * cols, cols), cols)
    to_partner(0, part.at[pl.ds(there, mine)], inbox)
    to_partner(1, tokv.at[pl.ds(there, mine), slot_cols], near)
    to_partner(2, gains.at[d], gains.at[d])

    home = home_is(grid)

    def spread_weights():
        for c in range(per):
            block = wov.at[:, pl.ds(c * cols, cols)]
            target = d * per + c
            Sender(a2a_send.at[0]).put(block, outw.at[0, t], a2a_recv.at[0], target, d, when=target != t)

            @pl.when(target == t)
            def _(c=c):
                outw[0, t] = wov[:, c * cols : (c + 1) * cols]

    half_z = grid.nz // 2

    def spread_planes():
        for k in range(half_z):
            block = wo.at[1, :, pl.ds(k * 4 * cols, 4 * cols)]
            level = d * half_z + k
            Sender(hub_send).put(block, hub.at[grid.z], hub_recv, level * 4 + lax.rem(t, 4), d, when=level != grid.z)

            @pl.when(level == grid.z)
            def _(block=block):
                pltpu.make_async_copy(block, hub.at[grid.z], hub_recv).start()

    def spread_plane():
        landed(hub, hub_recv, grid, home)
        for level in range(grid.nz):
            source = level * 4 + lax.rem(t, 4)
            for chip in (grid.xyp, grid.xp, grid.yp):
                block = hub.at[level, :, pl.ds(pl.multiple_of(lax.rem(chip, 4) * cols, cols), cols)]
                Sender(a2a_send.at[1]).put(block, outw.at[1, source], a2a_recv.at[1], chip, d, when=home)

            @pl.when(home)
            def _(level=level, source=source):
                outw[1, source] = hub[level, :, pl.ds(pl.multiple_of(lax.rem(t, 4) * cols, cols), cols)]

    def weights_left():
        away = jnp.logical_not(home)
        left(outw.at[0, 0:per], a2a_send.at[0], grid, away)
        left(outw.at[0, 0 : per - 1], a2a_send.at[0], grid, home)
        left(hub.at[0:half_z], hub_send, grid, away)
        left(hub.at[0 : half_z - 1], hub_send, grid, home)
        left(outw.at[1, 0 : 3 * grid.nz], a2a_send.at[1], grid, home)
        for layer in range(LAYERS):
            left(outw.at[layer], on_send.at[layer], grid, home)

    get_wo.wait()
    spread_weights()
    for i, w in enumerate(weights):
        to_partner(3, w.at[1], w1.at[d, pl.ds(i * HEAD, HEAD)])

    get_base.wait()
    get_ggain.wait()
    landed(inbox, pair_recv.at[0], grid)
    total = part[pl.ds(here, mine), :] + inbox[...]
    inv = lax.rsqrt(total[:, width : width + 1] / (feats * 2) + norm_floor)
    proj[...] = (inv * total[:, :width]).astype(jnp.bfloat16)

    landed(near, pair_recv.at[1], grid)
    own = tokv[pl.ds(here, mine), slot_cols].astype(jnp.float32)
    ours = home.astype(jnp.float32)
    current = own * ours + near[...].astype(jnp.float32) * (1.0 - ours)

    def forward_weights(layer):
        landed(outw.at[layer, 0 : (tp - 1 if layer == 0 else 3 * grid.nz)], a2a_recv.at[layer], grid, home)
        Sender(on_send.at[layer]).put(outw.at[layer], outw.at[layer], on_recv.at[layer], t, 1 - d, when=home)
        landed(outw.at[layer], on_recv.at[layer], grid, jnp.logical_not(home))

    def project_out(layer, mixed, current):
        mg[layer, t] = mixed

        def meanwhile():
            if layer == 0:
                spread_planes()

        def beside():
            if layer == 0:
                forward_weights(0)
                spread_plane()
            zero = jnp.zeros((HEAD, cols), we.dtype)
            for k in range(tp):
                block = outw[layer, k]
                top, bottom = pl.ds(k * PAIR, HEAD), pl.ds(k * PAIR + HEAD, HEAD)
                we[top, 0:cols] = block
                we[top, cols : 2 * cols] = zero
                we[bottom, 0:cols] = zero
                we[bottom, cols : 2 * cols] = block

        gather_heads(grid, mg.at[layer], m_send.at[layer], m_line.at[layer], m_plane.at[layer], meanwhile, beside)
        packed = jnp.concatenate([mg[layer, j] for j in range(tp)], axis=1)
        out = jnp.dot(packed, we[...], preferred_element_type=jnp.float32)
        out = jnp.concatenate([out[:, :cols], out[:, cols:]], axis=0)
        return (current + out).astype(jnp.bfloat16)

    seqs = min(mine, 64)
    get_state[0].wait()
    mixed = update_state(proj, base, ggain, 0, old, new, terms, reads, doubled, seqs)
    stream = project_out(0, mixed, current)

    lane = cols // 2
    for k in range(2):
        xg[t, k] = stream[:, k * lane : (k + 1) * lane]
    copy(w1.at[d], w1.at[d], 6).wait()
    landed(w1.at[1 - d], pair_recv.at[3], grid)
    landed(gains.at[1 - d], pair_recv.at[2], grid)
    acc[...] = jnp.zeros(acc.shape, jnp.float32)

    def use(block):
        half, at = block // per, pl.multiple_of(lax.rem(block, per) * cols, cols)
        floats = jnp.concatenate([xg[block, k] for k in range(2)], axis=1).astype(jnp.float32)
        normed = (floats * gains[half, 1:2, pl.ds(at, cols)]).astype(jnp.bfloat16)
        weight = w1[half, :, pl.ds(at, cols)]
        acc[:, 0:width] += lax.dot_general(normed, weight, NT, preferred_element_type=jnp.float32)
        squares = floats * floats
        for k in range(cols // PAIR):
            acc[:, width:] += squares[:, k * PAIR : (k + 1) * PAIR]

    tiles_left = gather_tiles(grid, xg, x_send, x_line, x_relayed, x_rest, use, lambda: forward_weights(1))
    inv = lax.rsqrt(jnp.sum(acc[:, width:], axis=1, keepdims=True) / (feats * 2) + norm_floor)
    proj[...] = (inv * acc[:, 0:width]).astype(jnp.bfloat16)

    get_state[1].wait()
    mixed = update_state(proj, base, ggain, 1, old, new, terms, reads, doubled, seqs)
    stream = project_out(1, mixed, stream.astype(jnp.float32))
    for k in range(2):
        tile[k] = stream[:, k * lane : (k + 1) * lane]
    spread_result(grid, tile, final, f_send, f_line, f_relayed, f_rest)

    tiles_left()
    left(part.at[pl.ds(there, mine)], pair_send.at[0], grid)
    left(near, pair_send.at[1], grid)
    left(gains.at[d], pair_send.at[2], grid)
    left(w1.at[d], pair_send.at[3], grid)
    weights_left()


def store_kernel(final, new, final_out, new_out, sems):
    ops = [pltpu.make_async_copy(new, new_out, sems.at[0]), pltpu.make_async_copy(final, final_out, sems.at[1])]
    for op in ops:
        op.start()
    for op in ops:
        op.wait()


def fast(tp, tokens, norm_gain, projections, decay_base, group_gain, output_proj, state):
    rows, feats = tokens.shape
    mine, per = rows // 2, tp // 2
    cols = feats // per
    width = 6 * HEAD
    lines = HEAD * HEAD // PAIR
    bf, f32 = jnp.bfloat16, jnp.float32
    shape, vmem, dma = jax.ShapeDtypeStruct, pltpu.VMEM, pltpu.SemaphoreType.DMA
    inside, anywhere = pl.BlockSpec(memory_space=pltpu.VMEM), pl.BlockSpec(memory_space=pl.ANY)
    turned = [jnp.swapaxes(w, 1, 2) for w in projections]
    flat = state.reshape(LAYERS, mine * lines, PAIR)
    outs = (shape((rows, feats), bf), shape(flat.shape, f32))
    final, new = pl.pallas_call(
        functools.partial(whole_kernel, tp),
        out_shape=(vmem((rows, feats), bf), vmem(flat.shape, f32)),
        in_specs=[pl.BlockSpec(memory_space=pltpu.HBM)] * 12,
        out_specs=(inside, inside),
        scratch_shapes=[
            vmem((rows, feats), bf), vmem((width, feats), bf), vmem((2, width, feats), bf), vmem((2, LAYERS, feats), f32),
            vmem((rows, width + PAIR), f32), vmem((mine, width + PAIR), f32), vmem((mine, width + PAIR), f32),
            vmem((mine, cols), bf),
            vmem((LAYERS, tp, HEAD, cols), bf), vmem((HEAD, feats), bf), vmem((tp // 4, HEAD, 4 * cols), bf), vmem((tp * PAIR, 2 * cols), bf), vmem((LAYERS, tp, mine // 2, PAIR), bf),
            vmem((tp, 2, mine, cols // 2), bf), vmem((2, mine, cols // 2), bf), vmem(flat.shape, f32),
            vmem((5, mine, PAIR), f32), vmem((mine, PAIR), f32), vmem((width, 2 * width), bf),
            vmem((mine, width), bf),
            vmem((LAYERS, HEAD), f32), vmem((LAYERS, HEAD), f32),
            dma((10,)), dma((4,)), dma((4,)), dma, dma, dma((LAYERS,)), dma((LAYERS,)), dma((LAYERS,)), dma((LAYERS,)),
            dma((LAYERS,)), dma((LAYERS, tp // 4)), dma((LAYERS,)),
            dma, dma((tp // 4,)), dma((tp // 4, 2)), dma((tp // 4,)),
            dma((2,)), dma((tp // 8, 2)), dma((tp // 8, 2, 2)), dma((2,)),
        ],
        compiler_params=pltpu.CompilerParams(collective_id=0, has_side_effects=True, vmem_limit_bytes=VMEM_LIMIT),
        name="whole",
    )(tokens, norm_gain, *turned, output_proj, decay_base, group_gain, flat)
    final, new = pl.pallas_call(
        store_kernel,
        out_shape=outs,
        in_specs=[inside, inside],
        out_specs=(anywhere, anywhere),
        scratch_shapes=[dma((2,))],
        compiler_params=pltpu.CompilerParams(vmem_limit_bytes=1024 * 1024),
        name="store",
    )(final, new)
    return (final, new.reshape(state.shape))


def step(tp, dp, tokens, norm_gain, *rest):
    projections, (decay_base, group_gain, output_proj, state) = rest[:6], rest[6:]
    rows, feats = tokens.shape
    fits = dp == 2 and tp % 16 == 0 and state.shape[2] == 1 and state.shape[1] % 64 == 0 and (feats * dp // tp) % 256 == 0
    if fits:
        return fast(tp, tokens, norm_gain, projections, decay_base, group_gain, output_proj, state)
    return shards(tokens, norm_gain, *rest)


def solution(mesh):
    return jax.shard_map(
        functools.partial(step, mesh.shape["tp"], mesh.shape["dp"]),
        mesh=mesh,
        in_specs=(
            P(None, "dp"),
            P(None, "dp"),
            P(None, "dp", "tp"),
            P(None, "dp", "tp"),
            P(None, "dp", "tp"),
            P(None, "dp", "tp"),
            P(None, "dp", "tp"),
            P(None, "dp", "tp"),
            P(None, "tp"),
            P(None, "tp"),
            P(None, "tp", "dp"),
            P(None, "dp", "tp", None),
        ),
        out_specs=(P(None, "dp"), P(None, "dp", "tp", None)),
        check_vma=False,
    )
```

```python
import functools
import math

import jax
import jax.numpy as jnp
from jax import lax
from jax.experimental import pallas as pl
from jax.experimental.pallas import tpu as pltpu
from jax.sharding import PartitionSpec as P

D = 4096
HEAD = 64
LAYERS = 2


norm_floor = 0.1
group_floor = 0.5


def recurrence(state_block, recept_heads, key_heads, value_heads, decay_heads, rate_heads):
    log_rate = -jax.nn.softplus(-decay_heads) - 0.5
    forget = jnp.exp(-jnp.exp(log_rate))
    learn_rate = jax.nn.sigmoid(rate_heads)
    unit_key = key_heads * lax.rsqrt(jnp.sum(key_heads * key_heads, axis=-1, keepdims=True) + 1.0)
    scaled = key_heads * learn_rate
    removed = jnp.einsum("bhvk,bhk->bhv", state_block, -unit_key, precision=lax.Precision.HIGHEST)
    updated = (
        state_block * forget[:, :, None, :]
        + removed[..., None] * (unit_key * learn_rate)[:, :, None, :]
        + value_heads[..., None] * scaled[:, :, None, :]
    )
    read_out = jnp.einsum("bhvk,bhk->bhv", updated, recept_heads, precision=lax.Precision.HIGHEST)
    centre = read_out - jnp.mean(read_out, axis=-1, keepdims=True)
    normal = centre * lax.rsqrt(jnp.mean(centre * centre, axis=-1, keepdims=True) + group_floor)
    return (updated, normal)


def shards(
    tokens,
    norm_gain,
    receptance,
    key_proj,
    value_proj,
    decay_proj,
    rate_proj,
    gate_proj,
    decay_base,
    group_gain,
    output_proj,
    state,
):
    local_rows = state.shape[1]
    first_row = lax.axis_index("dp") * local_rows
    local_heads = state.shape[2]
    current = tokens
    finals = []
    for section_index in range(LAYERS):
        floats = current.astype(jnp.float32)
        squares = jnp.sum(floats * floats, axis=1)
        normed = (floats * norm_gain[section_index]).astype(jnp.bfloat16)
        part_recept = jnp.dot(normed, receptance[section_index], preferred_element_type=jnp.float32)
        part_key = jnp.dot(normed, key_proj[section_index], preferred_element_type=jnp.float32)
        part_value = jnp.dot(normed, value_proj[section_index], preferred_element_type=jnp.float32)
        part_decay = jnp.dot(normed, decay_proj[section_index], preferred_element_type=jnp.float32)
        part_rate = jnp.dot(normed, rate_proj[section_index], preferred_element_type=jnp.float32)
        part_gate = jnp.dot(normed, gate_proj[section_index], preferred_element_type=jnp.float32)
        totals = lax.psum(squares, "dp")
        own_squares = lax.dynamic_slice_in_dim(totals, first_row, local_rows, 0)
        summed = (
            lax.psum_scatter(part_recept, "dp", scatter_dimension=0, tiled=True),
            lax.psum_scatter(part_key, "dp", scatter_dimension=0, tiled=True),
            lax.psum_scatter(part_value, "dp", scatter_dimension=0, tiled=True),
            lax.psum_scatter(part_decay, "dp", scatter_dimension=0, tiled=True),
            lax.psum_scatter(part_rate, "dp", scatter_dimension=0, tiled=True),
            lax.psum_scatter(part_gate, "dp", scatter_dimension=0, tiled=True),
        )
        inv_rms = lax.rsqrt(own_squares / D + norm_floor)

        def by_head(term):
            rounded = lax.optimization_barrier((inv_rms[:, None] * term).astype(jnp.bfloat16))
            return rounded.astype(jnp.float32).reshape(local_rows, local_heads, HEAD)

        decay_heads = by_head(summed[3]) + decay_base[section_index].reshape(1, local_heads, HEAD)
        updated, normal = recurrence(
            state[section_index].reshape(local_rows, local_heads, HEAD, HEAD),
            by_head(summed[0]),
            by_head(summed[1]),
            by_head(summed[2]),
            decay_heads,
            by_head(summed[4]),
        )
        finals.append(updated.reshape(local_rows, local_heads, HEAD * HEAD))
        gate_value = jax.nn.sigmoid(by_head(summed[5]).reshape(local_rows, local_heads * HEAD))
        mixed_heads = (
            normal.reshape(local_rows, local_heads * HEAD) * group_gain[section_index] * gate_value
        ).astype(jnp.bfloat16)
        weights_out = output_proj[section_index]

        def apply_out(piece, begin, weights_out=weights_out):
            return jnp.dot(piece, weights_out, preferred_element_type=jnp.float32)

        partial_out = apply_out(lax.all_gather(mixed_heads, "dp", axis=0, tiled=True), jnp.int32(0))
        total = lax.psum(partial_out, "tp")
        current = (floats + total).astype(jnp.bfloat16)
    return (current, jnp.stack(finals))


MESH = pl.DeviceIdType.MESH
NT = (((1,), (1,)), ((), ()))
PAIR = 2 * HEAD
VMEM_LIMIT = 57 * 1024 * 1024


class Grid:
    def __init__(self, tp):
        self.tp, self.nz, self.per = tp, tp // 4, tp // 2
        self.t, self.d = lax.axis_index("tp"), lax.axis_index("dp")
        self.z = self.t // 4
        x, y = lax.rem(self.t, 2), lax.rem(self.t // 2, 2)
        self.xp, self.yp = self.t + 1 - 2 * x, self.t + 2 - 4 * y
        self.xyp = self.xp + self.yp - self.t
        order = [sorted((k for k in range(self.nz) if k != z), key=lambda k: abs(k - z)) for z in range(self.nz)]
        self.line = []
        for k in range(self.nz - 1):
            level = order[0][k]
            for z in range(1, self.nz):
                level = jnp.where(self.z == z, order[z][k], level)
            self.line.append(level * 4 + lax.rem(self.t, 4))

    def over(self, base, chip):
        return base // 4 * 4 + lax.rem(chip, 4)

    def lots(self):
        return [self.t] + self.line


class Sender:
    def __init__(self, sem):
        self.sem = sem

    def put(self, src, dst, recv, t, d, when=None):
        op = pltpu.make_async_remote_copy(
            src_ref=src, dst_ref=dst, send_sem=self.sem, recv_sem=recv,
            device_id={"tp": t, "dp": d}, device_id_type=MESH,
        )
        if when is None:
            op.start()
        else:
            pl.when(when)(op.start)


def whole_of(ref, sem, grid):
    return pltpu.make_async_remote_copy(
        src_ref=ref, dst_ref=ref, send_sem=sem, recv_sem=sem,
        device_id={"tp": grid.xp, "dp": grid.d}, device_id_type=MESH,
    )


def landed(ref, recv, grid, when=None):
    op = whole_of(ref, recv, grid)
    if when is None:
        op.wait_recv()
    else:
        pl.when(when)(op.wait_recv)


def left(ref, send, grid, when=None):
    op = whole_of(ref, send, grid)
    if when is None:
        op.wait_send()
    else:
        pl.when(when)(op.wait_send)


def gather_heads(grid, buf, send, line, plane, meanwhile, beside):
    out = Sender(send)
    for chip in grid.line[::-1]:
        out.put(buf.at[grid.t], buf.at[grid.t], line.at[grid.z], chip, grid.d)
    for chip in (grid.xyp, grid.xp, grid.yp):
        out.put(buf.at[grid.t], buf.at[grid.t], plane, chip, grid.d)
    meanwhile()
    for block in grid.line:
        landed(buf.at[block], line.at[block // 4], grid)
        for chip in (grid.xyp, grid.xp, grid.yp):
            out.put(buf.at[block], buf.at[block], plane, chip, grid.d)
    beside()
    landed(buf.at[0 : 3 * grid.nz], plane, grid)
    left(buf.at[0 : 4 * grid.nz - 1], send, grid)


def gather_tiles(grid, buf, send, line, relayed, rest, use, after):
    out = Sender(send)

    def put(block, half, recv, chip):
        out.put(buf.at[block, half], buf.at[block, half], recv, chip, grid.d)

    def plane(block):
        level = block // 4
        put(block, 0, relayed.at[level, 0], grid.xp)
        put(block, 1, relayed.at[level, 1], grid.yp)
        put(block, 1, rest.at[level], grid.xp)
        put(block, 0, rest.at[level], grid.yp)

    def relay(lot):
        across, along, level = grid.over(lot, grid.xp), grid.over(lot, grid.yp), lot // 4
        landed(buf.at[across, 0], relayed.at[level, 0], grid)
        put(across, 0, rest.at[level], grid.yp)
        landed(buf.at[along, 1], relayed.at[level, 1], grid)
        put(along, 1, rest.at[level], grid.xp)

    for chip in grid.line:
        out.put(buf.at[grid.t], buf.at[grid.t], line.at[grid.z], chip, grid.d)
    plane(grid.t)
    last = grid.t
    for block in grid.line[:-1]:
        landed(buf.at[block], line.at[block // 4], grid)
        plane(block)
        relay(last)
        last = block
    block = grid.line[-1]
    landed(buf.at[block], line.at[block // 4], grid)
    for chip in (grid.xyp, grid.xp, grid.yp):
        out.put(buf.at[block], buf.at[block], rest.at[block // 4], chip, grid.d)
    relay(last)
    after()
    for k, lot in enumerate(grid.lots()):
        landed(buf.at[0 : 3 if k == grid.nz - 1 else 2], rest.at[lot // 4], grid)
        for block in (lot, grid.over(lot, grid.xp), grid.over(lot, grid.yp), grid.over(lot, grid.xyp)):
            use(block)

    def finish():
        left(buf.at[0 : 4 * grid.nz - 1], send, grid)

    return finish


def spread_result(grid, tile, final, send, line, relayed, rest):
    rows, lane = tile.shape[1], tile.shape[2]
    d, per, half_z = grid.d, grid.per, grid.nz // 2
    home = grid.t // per
    out, extra = Sender(send.at[0]), Sender(send.at[1])

    def place(block, r, half):
        at = pl.multiple_of((lax.rem(block, per) * 2 + half) * lane, lane)
        return final.at[pl.ds(pl.multiple_of(r * rows, rows), rows), pl.ds(at, lane)]

    def share(count):
        return final.at[pl.ds(0, count * rows // (2 * per))]

    def deep(block):
        return lax.rem(block // 4, half_z)

    def own(half, recv, chip, when=None):
        (out if when is None else extra).put(tile.at[half], place(grid.t, d, half), recv, chip, home, when)

    away = home != d
    level = deep(grid.t)
    for half in range(2):
        for chip in grid.line:
            own(half, line.at[level, d], chip)
    own(0, relayed.at[level, d, 0], grid.xp)
    own(1, relayed.at[level, d, 1], grid.yp)
    own(1, rest.at[0], grid.xp)
    own(0, rest.at[0], grid.yp)
    for half in range(2):
        own(half, rest.at[1], grid.t, away)

        @pl.when(home == d)
        def _(half=half):
            place(grid.t, d, half)[...] = tile[half]

    low = d * half_z
    lots = []
    for k in range(half_z):
        inside = low + lax.rem(grid.z - low + half_z + k, half_z)
        at = jnp.where(grid.z < low, low + k, jnp.where(grid.z >= low + half_z, low + half_z - 1 - k, inside))
        lots.append((at * 4 + lax.rem(grid.t, 4), at != grid.z))

    def put(block, r, half, recv, chip, far=None):
        (out if far is None else extra).put(place(block, r, half), place(block, r, half), recv, chip, d, far)

    def plane(lot, far):
        level = deep(lot)
        for r in range(2):
            landed(share(2), line.at[level, r], grid, far)
            put(lot, r, 0, relayed.at[level, r, 0], grid.xp, far)
            put(lot, r, 1, relayed.at[level, r, 1], grid.yp, far)
            put(lot, r, 1, rest.at[0], grid.xp, far)
            put(lot, r, 0, rest.at[0], grid.yp, far)

    def relay(lot):
        across, along, level = grid.over(lot, grid.xp), grid.over(lot, grid.yp), deep(lot)
        for r in range(2):
            landed(place(across, r, 0), relayed.at[level, r, 0], grid)
            put(across, r, 0, rest.at[0], grid.yp)
            landed(place(along, r, 1), relayed.at[level, r, 1], grid)
            put(along, r, 1, rest.at[0], grid.xp)

    def direct(lot):
        at = pl.multiple_of(lax.rem(lot, per) * 2 * lane, 2 * lane)
        for r in range(2):
            landed(share(2), line.at[deep(lot), r], grid)
            ref = final.at[pl.ds(r * rows, rows), pl.ds(at, 2 * lane)]
            for chip in (grid.xyp, grid.xp, grid.yp):
                out.put(ref, ref, rest.at[0], chip, d)

    for lot, far in lots[:-1]:
        plane(lot, far)
    direct(lots[-1][0])
    for lot, far in lots[:-1]:
        relay(lot)
    landed(share(8 * half_z + 4), rest.at[0], grid)
    landed(share(2), rest.at[1], grid, home_is(grid))
    left(share(2 * (grid.nz - 1) + 4 * half_z + 12), send.at[0], grid)
    left(share(2), send.at[1], grid, away)
    for lot, far in lots[:-1]:
        left(share(8), send.at[1], grid, far)


def home_is(grid):
    return grid.t // grid.per == grid.d


def iota(shape, axis):
    return lax.broadcasted_iota(jnp.int32, shape, axis)


def update_state(proj, base, ggain, layer, old, new, terms, reads, doubled, seqs):
    mine = proj.shape[0]
    lines = old.shape[1] // mine
    wide = jnp.dot(proj[...], doubled[...], preferred_element_type=jnp.float32)

    def piece(i):
        return wide[:, i * PAIR : (i + 1) * PAIR]

    def twice(row):
        return jnp.concatenate([row, row], axis=-1)

    recept, key, value, decay, rate, gate = [piece(i) for i in range(6)]
    scale = lax.rsqrt(jnp.sum(key * key, axis=-1, keepdims=True) * 0.5 + 1.0)
    forget = jnp.exp(-math.exp(-0.5) * jax.nn.sigmoid(decay + twice(base[layer : layer + 1, :])))
    learned = key * jax.nn.sigmoid(rate)
    for i, term in enumerate((key * (-scale * scale), forget, learned, recept, value)):
        terms[i] = term

    lane, col = iota((PAIR, PAIR), 0), iota((PAIR, PAIR), 1)
    same = (lane // HEAD == col // HEAD).astype(jnp.bfloat16)
    odd = ((lane < HEAD) & (lane % 2 == col // HEAD)).astype(jnp.bfloat16)
    turn = (lane // HEAD == col % 2).astype(jnp.bfloat16)
    both = jnp.concatenate([same, odd], axis=0)
    mask = (iota((lines, PAIR), 1) % HEAD) // 2 == iota((lines, PAIR), 0)

    def step(i, carry):
        begin = pl.multiple_of(i * seqs, seqs)
        first = pl.multiple_of(i * seqs * lines, seqs * lines)

        def spread(k):
            return jnp.broadcast_to(terms[k, pl.ds(begin, seqs), :][:, None, :], (seqs, lines, PAIR))

        state = old[layer, pl.ds(first, seqs * lines), :].reshape(seqs, lines, PAIR)
        product = (state * spread(0)).astype(jnp.bfloat16).reshape(seqs * lines, PAIR)
        chosen = jnp.where(mask[None], spread(4), 0.0).astype(jnp.bfloat16).reshape(seqs * lines, PAIR)
        rank = jnp.dot(jnp.concatenate([product, chosen], axis=1), both, preferred_element_type=jnp.float32)
        updated = state * spread(1) + rank.reshape(seqs, lines, PAIR) * spread(2)
        new[layer, pl.ds(first, seqs * lines), :] = updated.reshape(seqs * lines, PAIR)
        weighed = (updated * spread(3)).astype(jnp.bfloat16).reshape(seqs * lines, PAIR)
        read = jnp.dot(weighed, turn, preferred_element_type=jnp.float32).reshape(seqs, lines, PAIR)
        reads[pl.ds(begin, seqs), :] = jnp.sum(jnp.where(mask[None], read, 0.0), axis=1)
        return carry

    lax.fori_loop(0, mine // seqs, step, 0)
    read = reads[...]
    centre = read - jnp.mean(read, axis=-1, keepdims=True)
    normal = centre * lax.rsqrt(jnp.mean(centre * centre, axis=-1, keepdims=True) + group_floor)
    mixed = normal * twice(ggain[layer : layer + 1, :]) * jax.nn.sigmoid(gate)
    first = iota((mine // 2, PAIR), 1) < HEAD
    return jnp.where(first, mixed[0 : mine // 2], mixed[mine // 2 : mine]).astype(jnp.bfloat16)


def whole_kernel(
    tp, tok, gain, wr, wk, wv, wd, wa, wg, wo, base_in, ggain_in, state, final, new,
    tokv, w0, w1, gains, part, inbox, acc, near, outw, wov, hub, we, mg, xg, tile, old, terms, reads, doubled, proj, base, ggain,
    load, pair_send, pair_recv, hub_send, hub_recv, a2a_send, a2a_recv, on_send, on_recv, m_send, m_line, m_plane,
    x_send, x_line, x_relayed, x_rest, f_send, f_line, f_relayed, f_rest,
):
    grid = Grid(tp)
    t, d, per = grid.t, grid.d, grid.per
    rows, feats = tok.shape
    mine = rows // 2
    cols = near.shape[1]
    width = 6 * HEAD
    weights = (wr, wk, wv, wd, wa, wg)
    here, there = pl.multiple_of(d * mine, mine), pl.multiple_of((1 - d) * mine, mine)

    def copy(src, dst, number):
        return pltpu.make_async_copy(src, dst, load.at[number])

    get_there = copy(tok.at[pl.ds(there, mine)], tokv.at[pl.ds(there, mine)], 0)
    get_here = copy(tok.at[pl.ds(here, mine)], tokv.at[pl.ds(here, mine)], 1)
    get_gain = copy(gain, gains.at[d], 2)
    get_base, get_ggain = copy(base_in, base, 3), copy(ggain_in, ggain, 4)
    get_w0 = [copy(w.at[0], w0.at[pl.ds(i * HEAD, HEAD)], 5) for i, w in enumerate(weights)]
    get_w1 = [copy(w.at[1], w1.at[d, pl.ds(i * HEAD, HEAD)], 6) for i, w in enumerate(weights)]
    get_wo = copy(wo.at[0], wov, 9)
    get_state = [copy(state.at[k], old.at[k], 7 + k) for k in range(LAYERS)]
    for op in [get_there, get_gain] + get_w0 + [get_here, get_base, get_ggain]:
        op.start()

    barrier = pltpu.get_barrier_semaphore()
    for k in range(1, tp):
        for core in range(2):
            pl.semaphore_signal(barrier, inc=1, device_id={"tp": lax.rem(t + k, tp), "dp": core}, device_id_type=MESH)
    pl.semaphore_signal(barrier, inc=1, device_id={"tp": t, "dp": 1 - d}, device_id_type=MESH)
    for op in [get_wo, get_state[0]] + get_w1 + [get_state[1]]:
        op.start()
    source, column = iota((width, 2 * width), 0), iota((width, 2 * width), 1)
    wanted = column // PAIR * HEAD + column % HEAD
    doubled[...] = (source == wanted).astype(jnp.bfloat16)

    def project(begin):
        floats = tokv[pl.ds(begin, mine), :].astype(jnp.float32)
        part[pl.ds(begin, mine), width:] = jnp.broadcast_to(jnp.sum(floats * floats, axis=1, keepdims=True), (mine, PAIR))
        normed = (floats * gains[d, 0:1, :]).astype(jnp.bfloat16)
        part[pl.ds(begin, mine), 0:width] = lax.dot_general(normed, w0[...], NT, preferred_element_type=jnp.float32)

    get_there.wait()
    get_gain.wait()
    copy(w0, w0, 5).wait()
    project(there)
    get_here.wait()
    project(here)
    pl.semaphore_wait(barrier, 2 * tp - 1)

    def to_partner(number, src, dst):
        Sender(pair_send.at[number]).put(src, dst, pair_recv.at[number], t, 1 - d)

    slot = lax.rem(t, per)
    slot_cols = pl.ds(pl.multiple_of(slot * cols, cols), cols)
    to_partner(0, part.at[pl.ds(there, mine)], inbox)
    to_partner(1, tokv.at[pl.ds(there, mine), slot_cols], near)
    to_partner(2, gains.at[d], gains.at[d])

    home = home_is(grid)

    def spread_weights():
        for c in range(per):
            block = wov.at[:, pl.ds(c * cols, cols)]
            target = d * per + c
            Sender(a2a_send.at[0]).put(block, outw.at[0, t], a2a_recv.at[0], target, d, when=target != t)

            @pl.when(target == t)
            def _(c=c):
                outw[0, t] = wov[:, c * cols : (c + 1) * cols]

    half_z = grid.nz // 2

    def spread_planes():
        for k in range(half_z):
            block = wo.at[1, :, pl.ds(k * 4 * cols, 4 * cols)]
            level = d * half_z + k
            Sender(hub_send).put(block, hub.at[grid.z], hub_recv, level * 4 + lax.rem(t, 4), d, when=level != grid.z)

            @pl.when(level == grid.z)
            def _(block=block):
                pltpu.make_async_copy(block, hub.at[grid.z], hub_recv).start()

    def spread_plane():
        landed(hub, hub_recv, grid, home)
        for level in range(grid.nz):
            source = level * 4 + lax.rem(t, 4)
            for chip in (grid.xyp, grid.xp, grid.yp):
                block = hub.at[level, :, pl.ds(pl.multiple_of(lax.rem(chip, 4) * cols, cols), cols)]
                Sender(a2a_send.at[1]).put(block, outw.at[1, source], a2a_recv.at[1], chip, d, when=home)

            @pl.when(home)
            def _(level=level, source=source):
                outw[1, source] = hub[level, :, pl.ds(pl.multiple_of(lax.rem(t, 4) * cols, cols), cols)]

    def weights_left():
        away = jnp.logical_not(home)
        left(outw.at[0, 0:per], a2a_send.at[0], grid, away)
        left(outw.at[0, 0 : per - 1], a2a_send.at[0], grid, home)
        left(hub.at[0:half_z], hub_send, grid, away)
        left(hub.at[0 : half_z - 1], hub_send, grid, home)
        left(outw.at[1, 0 : 3 * grid.nz], a2a_send.at[1], grid, home)
        for layer in range(LAYERS):
            left(outw.at[layer], on_send.at[layer], grid, home)

    get_wo.wait()
    spread_weights()
    for i, w in enumerate(weights):
        to_partner(3, w.at[1], w1.at[d, pl.ds(i * HEAD, HEAD)])

    get_base.wait()
    get_ggain.wait()
    landed(inbox, pair_recv.at[0], grid)
    total = part[pl.ds(here, mine), :] + inbox[...]
    inv = lax.rsqrt(total[:, width : width + 1] / (feats * 2) + norm_floor)
    proj[...] = (inv * total[:, :width]).astype(jnp.bfloat16)

    landed(near, pair_recv.at[1], grid)
    own = tokv[pl.ds(here, mine), slot_cols].astype(jnp.float32)
    ours = home.astype(jnp.float32)
    current = own * ours + near[...].astype(jnp.float32) * (1.0 - ours)

    def forward_weights(layer):
        landed(outw.at[layer, 0 : (tp - 1 if layer == 0 else 3 * grid.nz)], a2a_recv.at[layer], grid, home)
        Sender(on_send.at[layer]).put(outw.at[layer], outw.at[layer], on_recv.at[layer], t, 1 - d, when=home)

    def weights_here(layer):
        landed(outw.at[layer], on_recv.at[layer], grid, jnp.logical_not(home))

    def project_out(layer, mixed, current):
        mg[layer, t] = mixed

        def meanwhile():
            if layer == 0:
                spread_planes()

        def beside():
            if layer == 0:
                forward_weights(0)
                spread_plane()
            weights_here(layer)
            zero = jnp.zeros((HEAD, cols), we.dtype)
            for k in range(tp):
                block = outw[layer, k]
                top, bottom = pl.ds(k * PAIR, HEAD), pl.ds(k * PAIR + HEAD, HEAD)
                we[top, 0:cols] = block
                we[top, cols : 2 * cols] = zero
                we[bottom, 0:cols] = zero
                we[bottom, cols : 2 * cols] = block

        gather_heads(grid, mg.at[layer], m_send.at[layer], m_line.at[layer], m_plane.at[layer], meanwhile, beside)
        packed = jnp.concatenate([mg[layer, j] for j in range(tp)], axis=1)
        out = jnp.dot(packed, we[...], preferred_element_type=jnp.float32)
        out = jnp.concatenate([out[:, :cols], out[:, cols:]], axis=0)
        return (current + out).astype(jnp.bfloat16)

    seqs = min(mine, 64)
    get_state[0].wait()
    mixed = update_state(proj, base, ggain, 0, old, new, terms, reads, doubled, seqs)
    stream = project_out(0, mixed, current)

    lane = cols // 2
    for k in range(2):
        xg[t, k] = stream[:, k * lane : (k + 1) * lane]
    copy(w1.at[d], w1.at[d], 6).wait()
    landed(w1.at[1 - d], pair_recv.at[3], grid)
    landed(gains.at[1 - d], pair_recv.at[2], grid)
    acc[...] = jnp.zeros(acc.shape, jnp.float32)

    def use(block):
        half, at = block // per, pl.multiple_of(lax.rem(block, per) * cols, cols)
        floats = jnp.concatenate([xg[block, k] for k in range(2)], axis=1).astype(jnp.float32)
        normed = (floats * gains[half, 1:2, pl.ds(at, cols)]).astype(jnp.bfloat16)
        weight = w1[half, :, pl.ds(at, cols)]
        acc[:, 0:width] += lax.dot_general(normed, weight, NT, preferred_element_type=jnp.float32)
        squares = floats * floats
        for k in range(cols // PAIR):
            acc[:, width:] += squares[:, k * PAIR : (k + 1) * PAIR]

    tiles_left = gather_tiles(grid, xg, x_send, x_line, x_relayed, x_rest, use, lambda: forward_weights(1))
    inv = lax.rsqrt(jnp.sum(acc[:, width:], axis=1, keepdims=True) / (feats * 2) + norm_floor)
    proj[...] = (inv * acc[:, 0:width]).astype(jnp.bfloat16)

    get_state[1].wait()
    mixed = update_state(proj, base, ggain, 1, old, new, terms, reads, doubled, seqs)
    stream = project_out(1, mixed, stream.astype(jnp.float32))
    for k in range(2):
        tile[k] = stream[:, k * lane : (k + 1) * lane]
    spread_result(grid, tile, final, f_send, f_line, f_relayed, f_rest)

    tiles_left()
    left(part.at[pl.ds(there, mine)], pair_send.at[0], grid)
    left(near, pair_send.at[1], grid)
    left(gains.at[d], pair_send.at[2], grid)
    left(w1.at[d], pair_send.at[3], grid)
    weights_left()


def store_kernel(final, new, final_out, new_out, sems):
    ops = [pltpu.make_async_copy(new, new_out, sems.at[0]), pltpu.make_async_copy(final, final_out, sems.at[1])]
    for op in ops:
        op.start()
    for op in ops:
        op.wait()


def fast(tp, tokens, norm_gain, projections, decay_base, group_gain, output_proj, state):
    rows, feats = tokens.shape
    mine, per = rows // 2, tp // 2
    cols = feats // per
    width = 6 * HEAD
    lines = HEAD * HEAD // PAIR
    bf, f32 = jnp.bfloat16, jnp.float32
    shape, vmem, dma = jax.ShapeDtypeStruct, pltpu.VMEM, pltpu.SemaphoreType.DMA
    inside, anywhere = pl.BlockSpec(memory_space=pltpu.VMEM), pl.BlockSpec(memory_space=pl.ANY)
    turned = [jnp.swapaxes(w, 1, 2) for w in projections]
    flat = state.reshape(LAYERS, mine * lines, PAIR)
    outs = (shape((rows, feats), bf), shape(flat.shape, f32))
    final, new = pl.pallas_call(
        functools.partial(whole_kernel, tp),
        out_shape=(vmem((rows, feats), bf), vmem(flat.shape, f32)),
        in_specs=[pl.BlockSpec(memory_space=pltpu.HBM)] * 12,
        out_specs=(inside, inside),
        scratch_shapes=[
            vmem((rows, feats), bf), vmem((width, feats), bf), vmem((2, width, feats), bf), vmem((2, LAYERS, feats), f32),
            vmem((rows, width + PAIR), f32), vmem((mine, width + PAIR), f32), vmem((mine, width + PAIR), f32),
            vmem((mine, cols), bf),
            vmem((LAYERS, tp, HEAD, cols), bf), vmem((HEAD, feats), bf), vmem((tp // 4, HEAD, 4 * cols), bf), vmem((tp * PAIR, 2 * cols), bf), vmem((LAYERS, tp, mine // 2, PAIR), bf),
            vmem((tp, 2, mine, cols // 2), bf), vmem((2, mine, cols // 2), bf), vmem(flat.shape, f32),
            vmem((5, mine, PAIR), f32), vmem((mine, PAIR), f32), vmem((width, 2 * width), bf),
            vmem((mine, width), bf),
            vmem((LAYERS, HEAD), f32), vmem((LAYERS, HEAD), f32),
            dma((10,)), dma((4,)), dma((4,)), dma, dma, dma((LAYERS,)), dma((LAYERS,)), dma((LAYERS,)), dma((LAYERS,)),
            dma((LAYERS,)), dma((LAYERS, tp // 4)), dma((LAYERS,)),
            dma, dma((tp // 4,)), dma((tp // 4, 2)), dma((tp // 4,)),
            dma((2,)), dma((tp // 8, 2)), dma((tp // 8, 2, 2)), dma((2,)),
        ],
        compiler_params=pltpu.CompilerParams(collective_id=0, has_side_effects=True, vmem_limit_bytes=VMEM_LIMIT),
        name="whole",
    )(tokens, norm_gain, *turned, output_proj, decay_base, group_gain, flat)
    final, new = pl.pallas_call(
        store_kernel,
        out_shape=outs,
        in_specs=[inside, inside],
        out_specs=(anywhere, anywhere),
        scratch_shapes=[dma((2,))],
        compiler_params=pltpu.CompilerParams(vmem_limit_bytes=1024 * 1024),
        name="store",
    )(final, new)
    return (final, new.reshape(state.shape))


def step(tp, dp, tokens, norm_gain, *rest):
    projections, (decay_base, group_gain, output_proj, state) = rest[:6], rest[6:]
    rows, feats = tokens.shape
    fits = dp == 2 and tp % 16 == 0 and state.shape[2] == 1 and state.shape[1] % 64 == 0 and (feats * dp // tp) % 256 == 0
    if fits:
        return fast(tp, tokens, norm_gain, projections, decay_base, group_gain, output_proj, state)
    return shards(tokens, norm_gain, *rest)


def solution(mesh):
    return jax.shard_map(
        functools.partial(step, mesh.shape["tp"], mesh.shape["dp"]),
        mesh=mesh,
        in_specs=(
            P(None, "dp"),
            P(None, "dp"),
            P(None, "dp", "tp"),
            P(None, "dp", "tp"),
            P(None, "dp", "tp"),
            P(None, "dp", "tp"),
            P(None, "dp", "tp"),
            P(None, "dp", "tp"),
            P(None, "tp"),
            P(None, "tp"),
            P(None, "tp", "dp"),
            P(None, "dp", "tp", None),
        ),
        out_specs=(P(None, "dp"), P(None, "dp", "tp", None)),
        check_vma=False,
    )
```
